256 devices in a mesh: fs: 32 (over z, y), tp: 8 (over x, core).
Axes of the slice: x: 4, y: 4, z: 8, core: 2. Of those that a mesh axis runs over, the one named last changes fastest.
Arguments:
- tokens: bfloat16 [32768, 2048], P('fs', 'tp'), may hold values from -6 to 6
- mixer_gain: float32 [2048], replicated, may hold values from 0.1 to 1.9
- conv_taps: bfloat16 [3, 1024], replicated, may hold values from -3.5 to 3.5
- outer_weight: bfloat16 [2048, 1024], P('fs', 'tp'), may hold values from -0.125 to 0.125
- inner_weight: bfloat16 [2048, 1024], P('fs', 'tp'), may hold values from -0.125 to 0.125
- value_weight: bfloat16 [2048, 1024], P('fs', 'tp'), may hold values from -0.125 to 0.125
- merge_weight: bfloat16 [1024, 2048], P('tp', 'fs'), may hold values from -0.375 to 0.375
- merge_gain: float32 [2048], replicated, may hold values from 0.1 to 1.9
- channel_gain: float32 [2048], replicated, may hold values from 0.1 to 1.9
- gate_weight: bfloat16 [2048, 5632], P('fs', 'tp'), may hold values from -0.125 to 0.125
- up_weight: bfloat16 [2048, 5632], P('fs', 'tp'), may hold values from -0.125 to 0.125
- down_weight: bfloat16 [5632, 2048], P('tp', 'fs'), may hold values from -0.15625 to 0.15625
- output_gain: float32 [2048], replicated, may hold values from 0.1 to 1.9
Outputs:
- layer_out: bfloat16 [32768, 2048], P('fs', 'tp')
The draws below stay inside these ranges and needn't reach their ends.
All inputs are finite; a program needn't handle non-finite values.
Results may differ from the reference program's by a relative error of at most 0.018.
Values may be sent and summed in bfloat16 or wider, within the bound.
No kernel may reach another device: no remote copies, remote signals or barrier semaphores. Data moves between devices by JAX's collectives and lax.ppermute only.
A program may use at most 128 MiB of HBM per device.

```python
import jax
import jax.numpy as jnp
from jax import lax

D = 2048
HEADS = 8
HEAD_DIM = 128
TAPS = 3
FF = 5632
SEQ = 1024
CONV_WIDTH = 1024
TOKENS = 32768
N_FS = 32
N_TP = 8


def strengthened(array, key, source, target, shards_of, factor):
    def block_of(axis_at):
        return (jnp.arange(array.shape[axis_at]) // (array.shape[axis_at] // shards_of)).reshape((-1,) + (1,) * (array.ndim - 1 - axis_at))

    first = jax.random.permutation(key, shards_of)[block_of(target)]
    far = (block_of(target) + shards_of // 2) % shards_of
    return jnp.where((block_of(source) == first) | (block_of(source) == far), factor * array, array)


def block_scale(stream_key, extent, cuts, smallest, largest):
    level, own = 1.0, jax.random.fold_in(stream_key, 6)
    for position, blocks in cuts:
        heights = jnp.exp(jax.random.uniform(jax.random.fold_in(own, position), (blocks,), jnp.float32, smallest / len(cuts), largest / len(cuts)))
        level = level * jnp.repeat(heights, extent[position] // blocks).reshape([-1 if axis == position else 1 for axis in range(len(extent))])
    return level


def gaussian(stream_key, dims, scale, bound, pieces=(), held_as=jnp.bfloat16):
    entries = scale * jax.random.normal(stream_key, dims, jnp.float32)
    if pieces:
        entries = entries * block_scale(stream_key, dims, pieces, -0.22, 0.18)
    return jnp.clip(entries, -bound, bound).astype(held_as)


def heavy_noise(own_key, shape, width, bound, cuts, heavy, dtype=jnp.bfloat16):
    array = width * jax.random.normal(own_key, shape, jnp.float32)
    if cuts:
        array = array * block_scale(own_key, shape, cuts, -0.22, 0.18)
    return jnp.clip(strengthened(array, jax.random.fold_in(own_key, 3), *heavy), -bound, bound).astype(dtype)


def setup_inputs(seed: int = 0) -> dict:
    arg_keys = jax.random.split(jax.random.key(seed), 14)
    return {
        "tokens": gaussian(arg_keys[0], (TOKENS, D), 1.0, 6.0, ((0, 32), (1, 8))),
        "mixer_gain": jnp.clip(1.0 + 0.18 * jax.random.normal(arg_keys[1], (D,), jnp.float32), 0.1, 1.9),
        "conv_taps": gaussian(arg_keys[2], (TAPS, CONV_WIDTH), TAPS ** -0.5, 3.5),
        "outer_weight": gaussian(arg_keys[3], (D, CONV_WIDTH), D ** -0.5, 0.125, ((0, 32), (1, 8))),
        "inner_weight": gaussian(arg_keys[4], (D, CONV_WIDTH), D ** -0.5, 0.125, ((0, 32), (1, 8))),
        "value_weight": gaussian(arg_keys[5], (D, CONV_WIDTH), D ** -0.5, 0.125, ((0, 32), (1, 8))),
        "merge_weight": heavy_noise(arg_keys[6], (CONV_WIDTH, D), CONV_WIDTH ** -0.5, 0.375, ((0, 8), (1, 32)), (0, 1, 32, 2.75)),
        "merge_gain": jnp.clip(1.0 + 0.18 * jax.random.normal(arg_keys[7], (D,), jnp.float32), 0.1, 1.9),
        "channel_gain": jnp.clip(1.0 + 0.18 * jax.random.normal(arg_keys[8], (D,), jnp.float32), 0.1, 1.9),
        "gate_weight": gaussian(arg_keys[9], (D, FF), D ** -0.5, 0.125, ((0, 32), (1, 8))),
        "up_weight": gaussian(arg_keys[10], (D, FF), D ** -0.5, 0.125, ((0, 32), (1, 8))),
        "down_weight": heavy_noise(arg_keys[11], (FF, D), FF ** -0.5, 0.15625, ((0, 8), (1, 32)), (0, 1, 32, 2.75)),
        "output_gain": jnp.clip(1.0 + 0.18 * jax.random.normal(arg_keys[12], (D,), jnp.float32), 0.1, 1.9),
    }


EPS = 1e-06

def normalize(values):
    floats = values.astype(jnp.float32)
    return floats * lax.rsqrt(lax.optimization_barrier(jnp.mean(floats * floats, axis=-1, keepdims=True)) + EPS)

def causal_taps(signal, taps):
    length = signal.shape[0]
    padded = jnp.pad(signal, ((2, 0), (0, 0)))
    return taps[0] * padded[:length] + taps[1] * padded[1:length + 1] + taps[2] * padded[2:]

def blocked_sum(hidden, weight):
    length = hidden.shape[0]
    block_rows = hidden.shape[1] // N_TP
    left = hidden.astype(jnp.float32).reshape(length, N_TP, block_rows)
    right = weight.astype(jnp.float32).reshape(N_TP, block_rows, weight.shape[1])
    partials = jnp.einsum('sbc,bcd->bsd', left, right)
    rounded = lax.optimization_barrier(partials.astype(jnp.bfloat16)).astype(jnp.float32)
    return lax.optimization_barrier(jnp.sum(rounded, axis=0)).astype(jnp.bfloat16)

def reference(tokens, mixer_gain, conv_taps, outer_weight, inner_weight, value_weight, merge_weight, merge_gain, channel_gain, gate_weight, up_weight, down_weight, output_gain):
    taps_float = conv_taps.astype(jnp.float32)

    def one_sequence(rows):
        normed = (normalize(rows) * mixer_gain).astype(jnp.bfloat16)
        outer = jnp.dot(normed, outer_weight, preferred_element_type=jnp.float32)
        inner = jnp.dot(normed, inner_weight, preferred_element_type=jnp.float32)
        value = jnp.dot(normed, value_weight, preferred_element_type=jnp.float32)
        conv = causal_taps(inner * value, taps_float)
        gated = (outer * conv).reshape(rows.shape[0], HEADS, HEAD_DIM)
        mixed = normalize(gated).reshape(rows.shape[0], CONV_WIDTH).astype(jnp.bfloat16)
        merged = blocked_sum(mixed, merge_weight)
        first = (rows.astype(jnp.float32) + normalize(merged) * merge_gain).astype(jnp.bfloat16)
        normed2 = (normalize(first) * channel_gain).astype(jnp.bfloat16)
        gate = jnp.dot(normed2, gate_weight, preferred_element_type=jnp.float32)
        upward = jnp.dot(normed2, up_weight, preferred_element_type=jnp.float32)
        hidden = (jax.nn.silu(gate) * upward).astype(jnp.bfloat16)
        down = blocked_sum(hidden, down_weight)
        return (first.astype(jnp.float32) + normalize(down) * output_gain).astype(jnp.bfloat16)
    outputs = lax.map(one_sequence, tokens.reshape(N_FS, SEQ, D))
    return outputs.reshape(TOKENS, D)
```

```python
import jax
import jax.numpy as jnp
from jax import lax
from jax.experimental import pallas as pl
from jax.experimental.pallas import tpu as pltpu
from jax.sharding import Mesh
from jax.sharding import PartitionSpec as P

TP = ("tp_0", "tp_1")
FS = ("fs_0", "fs_1")
EPS = 1e-06
HALO = 32
F32 = jnp.float32
BF16 = jnp.bfloat16


def shift(value, axis, by):
    n = lax.axis_size(axis)
    return lax.ppermute(value, axis, [(i, (i + by) % n) for i in range(n)])


def copy_for_each(value, axis):
    n = lax.axis_size(axis)
    return lax.all_to_all(
        jnp.broadcast_to(value[None], (n, *value.shape)), axis, 0, 0, tiled=True
    )


def around(value, axis):
    half = value.shape[0] // 2
    left = shift(value, axis, 1)
    right = shift(value, axis, -1)
    far_low = shift(left[:half], axis, 1)
    far_high = shift(right[half:], axis, -1)
    return value, left, right, far_low, far_high


def scatter_sum(own, to_right, to_left, keep_right, keep_left):
    half = own.shape[0] // 2
    from_left = shift(to_right, "tp_0", 1)
    from_right = shift(to_left, "tp_0", -1)
    add = lambda a, b: (a.astype(F32) + b.astype(F32)).astype(BF16)
    low = shift(add(keep_right, from_left[:half]), "tp_0", 1)
    high = shift(add(keep_left, from_right[:half]), "tp_0", -1)
    top = own[:half].astype(F32) + from_right[half:].astype(F32) + low.astype(F32)
    bottom = own[half:].astype(F32) + from_left[half:].astype(F32) + high.astype(F32)
    return jnp.concatenate([top, bottom], axis=0).astype(BF16)


def put_pieces(j, half, block, own, to_right, to_left, keep_right, keep_left, rows):
    if j == 0:
        own[rows, :] = block
    elif j == 1:
        if half == 0:
            keep_right[...] = block
        else:
            to_right[rows, :] = block
    elif j == 2:
        if half == 0:
            to_right[: block.shape[0], :] = block
        else:
            to_left[: block.shape[0], :] = block
    else:
        if half == 0:
            to_left[block.shape[0] :, :] = block
        else:
            keep_left[...] = block


def dot_nt(a, b):
    return lax.dot_general(a, b, (((1,), (1,)), ((), ())), preferred_element_type=F32)


def mixer_kernel(
    place, own, left, right, low, high, mine, other, taps, gain,
    o_own, o_right, o_left, o_keep_right, o_keep_left,
    weights, normed, outer, signal, sems,
):
    x, k = place[0], place[1]
    copies = []
    for side, source in enumerate((mine, other)):
        slot = k if side == 0 else 1 - k
        for y in range(4):
            for z in range(8):
                copies.append(
                    pltpu.make_async_copy(
                        source.at[y, z],
                        weights.at[slot, pl.ds((z * 4 + y) * 64, 64), :],
                        sems.at[side * 32 + y * 8 + z],
                    )
                )
    for copy in copies:
        copy.start()
    rows = normed.shape[0]
    half = rows // 2
    positions = [lax.rem(x + j, 4) for j in range(4)]
    for i in range(2):
        r = slice(i * half, (i + 1) * half)
        blocks = [own[r, :], right[r, :], (low if i == 0 else high)[...], left[r, :]]
        floats = [b.astype(F32) for b in blocks]
        squares = sum(jnp.sum(f * f, axis=1, keepdims=True) for f in floats)
        factor = lax.rsqrt(squares * (1.0 / 2048) + EPS)
        for j in range(4):
            g = gain[pl.ds(positions[j], 1), :]
            start = pl.multiple_of(positions[j] * 512, 512)
            normed[r, pl.ds(start, 512)] = (floats[j] * factor * g).astype(BF16)
    for copy in copies:
        copy.wait()
    signal[0:8, :] = jnp.zeros((8, 256), F32)
    for c in range(2):
        ch = slice(c * 128, (c + 1) * 128)
        for i in range(2):
            r = slice(i * half, (i + 1) * half)
            product = jnp.dot(normed[r, :], weights[c, :, 0:384], preferred_element_type=F32)
            outer[r, ch] = product[:, 0:128]
            signal[8 + i * half : 8 + (i + 1) * half, ch] = product[:, 128:256] * product[:, 256:384]
    mixed = []
    base = pl.multiple_of(k * HALO, HALO)
    for c in range(2):
        ch = slice(c * 128, (c + 1) * 128)
        s = signal[pl.ds(base, 520), ch]
        t = taps[:, ch]
        conv = t[0:1] * s[6:518] + t[1:2] * s[7:519] + t[2:3] * s[8:520]
        gated = outer[pl.ds(base, 512), ch] * conv
        scale = lax.rsqrt(jnp.mean(gated * gated, axis=1, keepdims=True) + EPS)
        mixed.append((gated * scale).astype(BF16))
    mixed = jnp.concatenate(mixed, axis=1)
    for j in range(4):
        start = pl.multiple_of(positions[j] * 512, 512)
        for zz in range(2):
            n = pl.ds(start + zz * 256, 256)
            w = jnp.concatenate([weights[0, n, 384:512], weights[1, n, 384:512]], axis=1)
            share = dot_nt(mixed, w).astype(BF16)
            cols = slice(zz * 256, (zz + 1) * 256)
            for h in range(2):
                put_pieces(
                    j, h, share[h * 256 : (h + 1) * 256],
                    *(ref.at[:, cols] for ref in (o_own, o_right, o_left, o_keep_right, o_keep_left)),
                    slice(h * 256, (h + 1) * 256),
                )


def forward_kernel(
    place, t_own, t_left, t_right, t_far, m_own, m_left, m_right, m_low, m_high, *rest
):
    pieces, rest = rest[:10], rest[10:]
    merge_gain, channel_gain = rest[:2]
    o_own, o_right, o_left, o_keep_right, o_keep_left, o_first = rest[2:8]
    weights, normed, hidden, sems = rest[8:]
    x, k, y = place[0], place[1], place[2]
    copies = []
    for side in range(2):
        slot = k if side == 0 else 1 - k
        for q, (turn, z0, zs) in enumerate(((0, 0, 8), (3, 0, 8), (1, 0, 8), (2, 0, 4), (2, 4, 4))):
            at = lax.rem(y + turn, 4)
            for z in range(zs):
                row = pl.multiple_of(((z0 + z) * 4 + at) * 64, 64)
                copies.append(
                    pltpu.make_async_copy(
                        pieces[side * 5 + q].at[z],
                        weights.at[slot, pl.ds(row, 64), :],
                        sems.at[side * 32 + (24 + z0 if q > 2 else q * 8) + z],
                    )
                )
    for copy in copies:
        copy.start()
    positions = [lax.rem(x + j, 4) for j in range(4)]
    base = pl.multiple_of(k * HALO, HALO)
    lane = lax.broadcasted_iota(jnp.int32, (256, 128), 1)
    for i in range(2):
        r = slice(i * 256, (i + 1) * 256)
        tr = pl.ds(base + i * 256, 256)
        merged = [b.astype(F32) for b in (m_own[r, :], m_right[r, :], (m_low if i == 0 else m_high)[...], m_left[r, :])]
        toks = [b[tr, :].astype(F32) for b in (t_own, t_right, t_far, t_left)]
        squares = sum(jnp.sum(f * f, axis=1, keepdims=True) for f in merged)
        factor = lax.rsqrt(squares * (1.0 / 2048) + EPS)
        first = []
        for j in range(4):
            g = merge_gain[pl.ds(positions[j], 1), :]
            first.append((toks[j] + merged[j] * factor * g).astype(BF16))
        o_first[r, :] = first[0]
        first = [f.astype(F32) for f in first]
        squares = sum(jnp.sum(f * f, axis=1, keepdims=True) for f in first)
        factor = lax.rsqrt(squares * (1.0 / 2048) + EPS)
        for j in range(4):
            g = channel_gain[pl.ds(positions[j], 1), :]
            start = pl.multiple_of(positions[j] * 512, 512)
            normed[r, pl.ds(start, 512)] = (first[j] * factor * g).astype(BF16)
    for copy in copies:
        copy.wait()
    for i in range(2):
        r = slice(i * 256, (i + 1) * 256)
        for c in range(2):
            both = jnp.dot(normed[r, :], weights[c, :, 0:1408], preferred_element_type=F32)
            gate, up, tail = both[:, 0:640], both[:, 640:1280], both[:, 1280:1408]
            hidden[r, c * 768 : c * 768 + 640] = (gate / (1.0 + jnp.exp(-gate)) * up).astype(BF16)
            other = pltpu.roll(tail, 64, 1)
            last = jnp.where(lane < 64, tail / (1.0 + jnp.exp(-tail)) * other, 0.0)
            hidden[r, c * 768 + 640 : (c + 1) * 768] = last.astype(BF16)
        for j in range(4):
            for zz in range(2):
                n = pl.ds(pl.multiple_of(positions[j] * 512, 512) + zz * 256, 256)
                share = dot_nt(hidden[r, 0:768], weights[0, n, 1408:2176])
                share += dot_nt(hidden[r, 768:1536], weights[1, n, 1408:2176])
                cols = slice(zz * 256, (zz + 1) * 256)
                put_pieces(
                    j, i, share.astype(BF16),
                    *(ref.at[:, cols] for ref in (o_own, o_right, o_left, o_keep_right, o_keep_left)),
                    r,
                )


VM = pl.BlockSpec(memory_space=pltpu.VMEM)
SM = pl.BlockSpec(memory_space=pltpu.SMEM)
HB = pl.BlockSpec(memory_space=pltpu.HBM)
SHARES = [
    jax.ShapeDtypeStruct((512, 512), BF16),
    jax.ShapeDtypeStruct((512, 512), BF16),
    jax.ShapeDtypeStruct((512, 512), BF16),
    jax.ShapeDtypeStruct((256, 512), BF16),
    jax.ShapeDtypeStruct((256, 512), BF16),
]


def shards(
    tokens, mixer_gain, conv_taps, outer_weight, inner_weight, value_weight, merge_weight,
    merge_gain, channel_gain, gate_weight, up_weight, down_weight, output_gain,
):
    x, k, y = lax.axis_index("tp_0"), lax.axis_index("tp_1"), lax.axis_index("fs_1")
    place = jnp.stack([x, k, y]).astype(jnp.int32)
    span = 512 + HALO

    first_weights = jnp.concatenate([outer_weight, inner_weight, value_weight, merge_weight.T], axis=1)
    second_weights = jnp.concatenate(
        [
            gate_weight[:, :640], up_weight[:, :640], gate_weight[:, 640:], up_weight[:, 640:],
            down_weight.T, jnp.zeros((64, 64), BF16),
        ],
        axis=1,
    )

    kept = lax.dynamic_slice_in_dim(tokens, k * (512 - HALO), span, 0)
    given = lax.dynamic_slice_in_dim(tokens, (1 - k) * (512 - HALO), span, 0)
    taken = shift(given, "tp_1", 1)
    block = jnp.where(k == 0, jnp.concatenate([kept, taken], 1), jnp.concatenate([taken, kept], 1))
    t_own, t_left, t_right, t_low, t_high = around(block, "tp_0")

    near = copy_for_each(copy_for_each(first_weights, "fs_0"), "fs_1")
    near_other = shift(near, "tp_1", 1)

    planes = copy_for_each(second_weights, "fs_0")
    far = around(planes, "fs_1")
    far_other = [shift(part, "tp_1", 1) for part in far]

    own_taps = lax.dynamic_slice_in_dim(conv_taps, x * 256, 256, 1).astype(F32)
    pieces = pl.pallas_call(
        mixer_kernel,
        out_shape=SHARES,
        in_specs=[SM] + [VM] * 5 + [HB] * 2 + [VM] * 2,
        out_specs=[VM] * 5,
        scratch_shapes=[
            pltpu.VMEM((2, 2048, 512), BF16),
            pltpu.VMEM((span, 2048), BF16),
            pltpu.VMEM((span, 256), F32),
            pltpu.VMEM((span + 8, 256), F32),
            pltpu.SemaphoreType.DMA((64,)),
        ],
        compiler_params=pltpu.CompilerParams(vmem_limit_bytes=40 * 2**20),
        cost_estimate=pl.CostEstimate(flops=2_300_000_000, bytes_accessed=9_000_000, transcendentals=0),
    )(place, t_own, t_left, t_right, t_low, t_high, near, near_other, own_taps, mixer_gain.reshape(4, 512))
    merged = scatter_sum(*pieces)
    gathered = around(merged, "tp_0")

    *pieces, first = pl.pallas_call(
        forward_kernel,
        out_shape=SHARES + [jax.ShapeDtypeStruct((512, 512), BF16)],
        in_specs=[SM] + [VM] * 9 + [HB] * 10 + [VM] * 2,
        out_specs=[VM] * 6,
        scratch_shapes=[
            pltpu.VMEM((2, 2048, 2176), BF16),
            pltpu.VMEM((512, 2048), BF16),
            pltpu.VMEM((512, 1536), BF16),
            pltpu.SemaphoreType.DMA((64,)),
        ],
        compiler_params=pltpu.CompilerParams(vmem_limit_bytes=52 * 2**20),
        cost_estimate=pl.CostEstimate(flops=9_500_000_000, bytes_accessed=24_000_000, transcendentals=0),
    )(
        place, t_own, t_left, t_right, jnp.concatenate([t_low, t_high], 0), *gathered, *far, *far_other,
        merge_gain.reshape(4, 512), channel_gain.reshape(4, 512),
    )
    down = scatter_sum(*pieces).astype(F32)
    squares = jnp.sum(down * down, axis=1).reshape(4, 128)
    total = squares + shift(squares, "tp_0", 1) + shift(squares, "tp_0", -1) + shift(squares, "tp_0", 2)
    factor = lax.rsqrt(total.reshape(512, 1) / 2048 + EPS)
    own_gain = lax.dynamic_slice_in_dim(output_gain, x * 512, 512)
    result = (first.astype(F32) + down * factor * own_gain).astype(BF16)
    kept = lax.dynamic_slice_in_dim(result, k * 256, 256, 1)
    given = lax.dynamic_slice_in_dim(result, (1 - k) * 256, 256, 1)
    taken = shift(given, "tp_1", 1)
    return jnp.where(k == 0, jnp.concatenate([kept, taken], 0), jnp.concatenate([taken, kept], 0))


def solution(mesh):
    finer = Mesh(mesh.devices.reshape(8, 4, 4, 2), ("fs_0", "fs_1", "tp_0", "tp_1"))
    wide, tall = P(FS, TP), P(TP, FS)
    placed = (wide, P(), P(), wide, wide, wide, tall, P(), P(), wide, wide, tall, P())
    return jax.shard_map(shards, mesh=finer, in_specs=placed, out_specs=P(FS, TP), check_vma=False)
```

```python
import jax
import jax.numpy as jnp
from jax import lax
from jax.experimental import pallas as pl
from jax.experimental.pallas import tpu as pltpu
from jax.sharding import Mesh
from jax.sharding import PartitionSpec as P

TP = ("tp_0", "tp_1")
FS = ("fs_0", "fs_1")
EPS = 1e-06
HALO = 32
F32 = jnp.float32
BF16 = jnp.bfloat16


def shift(value, axis, by):
    n = lax.axis_size(axis)
    return lax.ppermute(value, axis, [(i, (i + by) % n) for i in range(n)])


def around(value, axis):
    half = value.shape[0] // 2
    left = shift(value, axis, 1)
    right = shift(value, axis, -1)
    far_low = shift(left[:half], axis, 1)
    far_high = shift(right[half:], axis, -1)
    return value, left, right, far_low, far_high


def around_eight(value, axis):
    half = value.shape[0] // 2
    left, right, blocks = value, value, [value]
    for _ in range(3):
        left, right = shift(left, axis, 1), shift(right, axis, -1)
        blocks += [left, right]
    return *blocks, shift(left[:half], axis, 1), shift(right[half:], axis, -1)


def scatter_sum(own, to_right, to_left, keep_right, keep_left):
    half = own.shape[0] // 2
    from_left = shift(to_right, "tp_0", 1)
    from_right = shift(to_left, "tp_0", -1)
    add = lambda a, b: (a.astype(F32) + b.astype(F32)).astype(BF16)
    low = shift(add(keep_right, from_left[:half]), "tp_0", 1)
    high = shift(add(keep_left, from_right[:half]), "tp_0", -1)
    low, high, from_left, from_right = lax.optimization_barrier((low, high, from_left, from_right))
    top = own[:half].astype(F32) + from_right[half:].astype(F32) + low.astype(F32)
    bottom = own[half:].astype(F32) + from_left[half:].astype(F32) + high.astype(F32)
    return jnp.concatenate([top, bottom], axis=0).astype(BF16)


def put_pieces(j, half, block, own, to_right, to_left, keep_right, keep_left, rows):
    if j == 0:
        own[rows, :] = block
    elif j == 1:
        if half == 0:
            keep_right[...] = block
        else:
            to_right[rows, :] = block
    elif j == 2:
        if half == 0:
            to_right[: block.shape[0], :] = block
        else:
            to_left[: block.shape[0], :] = block
    else:
        if half == 0:
            to_left[block.shape[0] :, :] = block
        else:
            keep_left[...] = block


def dot_nt(a, b):
    return lax.dot_general(a, b, (((1,), (1,)), ((), ())), preferred_element_type=F32)


ORDER_Z = (0, 7, 1, 6, 2, 5, 3, 4)
PARTS_Y = ((0, 0, 8), (3, 0, 8), (1, 0, 8), (2, 0, 4), (2, 4, 8))


def mixer_kernel(
    place, own, left, right, low, high, *rest
):
    pieces, rest = rest[:10], rest[10:]
    taps, gain, o_own, o_right, o_left, o_keep_right, o_keep_left = rest[:7]
    weights, normed, outer, signal, sems = rest[7:]
    x, k, y, z = place[0], place[1], place[2], place[3]
    copies = []
    for side in range(2):
        slot = k if side == 0 else 1 - k
        for q, (turn, begin, end) in enumerate(PARTS_Y):
            at = lax.rem(y + turn, 4)
            for b in range(begin, end):
                row = pl.multiple_of((lax.rem(z + ORDER_Z[b], 8) * 4 + at) * 64, 64)
                copies.append(
                    pltpu.make_async_copy(
                        pieces[side * 5 + q].at[b - begin],
                        weights.at[slot, pl.ds(row, 64), :],
                        sems.at[len(copies)],
                    )
                )
    for copy in copies:
        copy.start()
    rows = normed.shape[0]
    half = rows // 2
    positions = [lax.rem(x + j, 4) for j in range(4)]
    for i in range(2):
        r = slice(i * half, (i + 1) * half)
        blocks = [own[r, :], right[r, :], (low if i == 0 else high)[...], left[r, :]]
        floats = [b.astype(F32) for b in blocks]
        squares = sum(jnp.sum(f * f, axis=1, keepdims=True) for f in floats)
        factor = lax.rsqrt(squares * (1.0 / 2048) + EPS)
        for j in range(4):
            g = gain[pl.ds(positions[j], 1), :]
            start = pl.multiple_of(positions[j] * 512, 512)
            normed[r, pl.ds(start, 512)] = (floats[j] * factor * g).astype(BF16)
    for copy in copies:
        copy.wait()
    signal[0:8, :] = jnp.zeros((8, 256), F32)

    @pl.loop(0, 2)
    def _(i):
        at = pl.multiple_of(i * half, 16)
        for c in range(2):
            ch = slice(c * 128, (c + 1) * 128)
            product = jnp.dot(normed[pl.ds(at, half), :], weights[c, :, 0:384], preferred_element_type=F32)
            outer[pl.ds(at, half), ch] = product[:, 0:128]
            signal[pl.ds(at + 8, half), ch] = product[:, 128:256] * product[:, 256:384]

    mixed = []
    base = pl.multiple_of(k * HALO, HALO)
    for c in range(2):
        ch = slice(c * 128, (c + 1) * 128)
        s = signal[pl.ds(base, 520), ch]
        t = taps[:, ch]
        conv = t[0:1] * s[6:518] + t[1:2] * s[7:519] + t[2:3] * s[8:520]
        gated = outer[pl.ds(base, 512), ch] * conv
        scale = lax.rsqrt(jnp.mean(gated * gated, axis=1, keepdims=True) + EPS)
        mixed.append((gated * scale).astype(BF16))
    mixed = jnp.concatenate(mixed, axis=1)
    for j in range(4):
        start = pl.multiple_of(positions[j] * 512, 512)
        for zz in range(2):
            n = pl.ds(start + zz * 256, 256)
            w = jnp.concatenate([weights[0, n, 384:512], weights[1, n, 384:512]], axis=1)
            share = dot_nt(mixed, w).astype(BF16)
            cols = slice(zz * 256, (zz + 1) * 256)
            for h in range(2):
                put_pieces(
                    j, h, share[h * 256 : (h + 1) * 256],
                    *(ref.at[:, cols] for ref in (o_own, o_right, o_left, o_keep_right, o_keep_left)),
                    slice(h * 256, (h + 1) * 256),
                )


def norm_kernel(
    place, t_own, t_left, t_right, t_far, m_own, m_left, m_right, m_low, m_high,
    merge_gain, channel_gain, normed, o_first,
):
    x, k = place[0], place[1]
    positions = [lax.rem(x + j, 4) for j in range(4)]
    base = pl.multiple_of(k * HALO, HALO)
    for i in range(2):
        r = slice(i * 256, (i + 1) * 256)
        tr = pl.ds(base + i * 256, 256)
        merged = [b.astype(F32) for b in (m_own[r, :], m_right[r, :], (m_low if i == 0 else m_high)[...], m_left[r, :])]
        toks = [b[tr, :].astype(F32) for b in (t_own, t_right, t_far, t_left)]
        squares = sum(jnp.sum(f * f, axis=1, keepdims=True) for f in merged)
        factor = lax.rsqrt(squares * (1.0 / 2048) + EPS)
        first = []
        for j in range(4):
            g = merge_gain[pl.ds(positions[j], 1), :]
            first.append((toks[j] + merged[j] * factor * g).astype(BF16))
        o_first[r, :] = first[0]
        first = [f.astype(F32) for f in first]
        squares = sum(jnp.sum(f * f, axis=1, keepdims=True) for f in first)
        factor = lax.rsqrt(squares * (1.0 / 2048) + EPS)
        for j in range(4):
            g = channel_gain[pl.ds(positions[j], 1), :]
            start = pl.multiple_of(positions[j] * 512, 512)
            normed[r, pl.ds(start, 512)] = (first[j] * factor * g).astype(BF16)


def pack_kernel(gate, up, down, out):
    out[:, 0:640] = gate[:, 0:640]
    out[:, 640:1280] = up[:, 0:640]
    out[:, 1280:1408] = jnp.concatenate([gate[:, 640:704], up[:, 640:704]], axis=1)
    out[:, 1408:2048] = down[:, 0:640]
    out[:, 2048:2176] = jnp.concatenate([down[:, 640:704], jnp.zeros((64, 64), BF16)], axis=1)


def forward_kernel(place, normed, weights, out):
    x = place[0]
    lane = lax.broadcasted_iota(jnp.int32, (256, 128), 1)

    @pl.loop(0, 2)
    def _(i):
        r = pl.ds(pl.multiple_of(i * 256, 256), 256)
        both = jnp.dot(normed[r, :], weights[:, 0:1408], preferred_element_type=F32)
        gate, up, tail = both[:, 0:640], both[:, 640:1280], both[:, 1280:1408]
        hidden = (gate / (1.0 + jnp.exp(-gate)) * up).astype(BF16)
        other = pltpu.roll(tail, 64, 1)
        last = jnp.where(lane < 64, tail / (1.0 + jnp.exp(-tail)) * other, 0.0)
        hidden = jnp.concatenate([hidden, last.astype(BF16)], axis=1)
        for j in range(4):
            start = pl.multiple_of(lax.rem(x + j, 4) * 512, 512)
            for zz in range(2):
                n = pl.ds(start + zz * 256, 256)
                out[j, r, zz * 256 : (zz + 1) * 256] = dot_nt(hidden, weights[n, 1408:2176]).astype(BF16)


VM = pl.BlockSpec(memory_space=pltpu.VMEM)
SM = pl.BlockSpec(memory_space=pltpu.SMEM)
HB = pl.BlockSpec(memory_space=pltpu.HBM)
SHARES = [
    jax.ShapeDtypeStruct((512, 512), BF16),
    jax.ShapeDtypeStruct((512, 512), BF16),
    jax.ShapeDtypeStruct((512, 512), BF16),
    jax.ShapeDtypeStruct((256, 512), BF16),
    jax.ShapeDtypeStruct((256, 512), BF16),
]


def shards(
    tokens, mixer_gain, conv_taps, outer_weight, inner_weight, value_weight, merge_weight,
    merge_gain, channel_gain, gate_weight, up_weight, down_weight, output_gain,
):
    x, k = lax.axis_index("tp_0"), lax.axis_index("tp_1")
    y, z = lax.axis_index("fs_1"), lax.axis_index("fs_0")
    place = jnp.stack([x, k, y, z]).astype(jnp.int32)
    span = 512 + HALO

    first_weights = jnp.concatenate([outer_weight, inner_weight, value_weight, merge_weight.T], axis=1)
    second_weights = pl.pallas_call(
        pack_kernel, out_shape=jax.ShapeDtypeStruct((64, 2176), BF16), in_specs=[VM] * 3, out_specs=VM
    )(gate_weight, up_weight, down_weight.T)
    second = lax.all_gather(second_weights, FS, axis=0, tiled=True)

    kept = lax.dynamic_slice_in_dim(tokens, k * (512 - HALO), span, 0)
    given = lax.dynamic_slice_in_dim(tokens, (1 - k) * (512 - HALO), span, 0)
    taken = shift(given, "tp_1", 1)
    block = jnp.where(k == 0, jnp.concatenate([kept, taken], 1), jnp.concatenate([taken, kept], 1))
    t_own, t_left, t_right, t_low, t_high = around(block, "tp_0")

    plane = around_eight(first_weights, "fs_0")
    plane = jnp.concatenate(plane, axis=0).reshape(8, 64, 512)
    near = around(plane, "fs_1")
    near_other = [shift(part, "tp_1", 1) for part in near]

    own_taps = lax.dynamic_slice_in_dim(conv_taps, x * 256, 256, 1).astype(F32)
    pieces = pl.pallas_call(
        mixer_kernel,
        out_shape=SHARES,
        in_specs=[SM] + [VM] * 5 + [HB] * 10 + [VM] * 2,
        out_specs=[VM] * 5,
        scratch_shapes=[
            pltpu.VMEM((2, 2048, 512), BF16),
            pltpu.VMEM((span, 2048), BF16),
            pltpu.VMEM((span, 256), F32),
            pltpu.VMEM((span + 8, 256), F32),
            pltpu.SemaphoreType.DMA((64,)),
        ],
        compiler_params=pltpu.CompilerParams(vmem_limit_bytes=40 * 2**20),
        cost_estimate=pl.CostEstimate(flops=2_300_000_000, bytes_accessed=9_000_000, transcendentals=0),
    )(place, t_own, t_left, t_right, t_low, t_high, *near, *near_other, own_taps, mixer_gain.reshape(4, 512))
    merged = scatter_sum(*pieces)
    gathered = around(merged, "tp_0")

    normed, first = pl.pallas_call(
        norm_kernel,
        out_shape=[jax.ShapeDtypeStruct((512, 2048), BF16), jax.ShapeDtypeStruct((512, 512), BF16)],
        in_specs=[SM] + [VM] * 11,
        out_specs=[VM] * 2,
        compiler_params=pltpu.CompilerParams(vmem_limit_bytes=32 * 2**20),
        cost_estimate=pl.CostEstimate(flops=30_000_000, bytes_accessed=6_500_000, transcendentals=0),
    )(
        place, t_own, t_left, t_right, jnp.concatenate([t_low, t_high], 0), *gathered,
        merge_gain.reshape(4, 512), channel_gain.reshape(4, 512),
    )
    forward = pl.pallas_call(
        forward_kernel,
        out_shape=jax.ShapeDtypeStruct((4, 512, 512), BF16),
        in_specs=[SM] + [VM] * 2,
        out_specs=VM,
        compiler_params=pltpu.CompilerParams(vmem_limit_bytes=40 * 2**20),
        cost_estimate=pl.CostEstimate(flops=4_500_000_000, bytes_accessed=13_000_000, transcendentals=0),
    )
    theirs = shift(forward(place, shift(normed, "tp_1", 1), second), "tp_1", 1).astype(F32)
    ours = forward(place, normed, second).astype(F32) + theirs
    ours = ours.astype(BF16)
    pieces = (
        ours[0],
        jnp.concatenate([ours[2, :256], ours[1, 256:]], 0),
        jnp.concatenate([ours[2, 256:], ours[3, :256]], 0),
        ours[1, :256],
        ours[3, 256:],
    )
    down = scatter_sum(*pieces).astype(F32)
    squares = jnp.sum(down * down, axis=1).reshape(4, 128)
    total = squares + shift(squares, "tp_0", 1) + shift(squares, "tp_0", -1) + shift(squares, "tp_0", 2)
    factor = lax.rsqrt(total.reshape(512, 1) / 2048 + EPS)
    own_gain = lax.dynamic_slice_in_dim(output_gain, x * 512, 512)
    result = (first.astype(F32) + down * factor * own_gain).astype(BF16)
    kept = lax.dynamic_slice_in_dim(result, k * 256, 256, 1)
    given = lax.dynamic_slice_in_dim(result, (1 - k) * 256, 256, 1)
    taken = shift(given, "tp_1", 1)
    return jnp.where(k == 0, jnp.concatenate([kept, taken], 0), jnp.concatenate([taken, kept], 0))


def solution(mesh):
    finer = Mesh(mesh.devices.reshape(8, 4, 4, 2), ("fs_0", "fs_1", "tp_0", "tp_1"))
    wide, tall = P(FS, TP), P(TP, FS)
    placed = (wide, P(), P(), wide, wide, wide, tall, P(), P(), wide, wide, tall, P())
    named = lambda *args: shards(*args)
    return jax.shard_map(named, mesh=finer, in_specs=placed, out_specs=P(FS, TP), check_vma=False)
```

```python
import jax
import jax.numpy as jnp
from jax import lax
from jax.experimental import pallas as pl
from jax.experimental.pallas import tpu as pltpu
from jax.sharding import Mesh
from jax.sharding import PartitionSpec as P

TP = ("tp_0", "tp_1")
FS = ("fs_0", "fs_1")
EPS = 1e-06
HALO = 32
F32 = jnp.float32
BF16 = jnp.bfloat16


def shift(value, axis, by):
    n = lax.axis_size(axis)
    return lax.ppermute(value, axis, [(i, (i + by) % n) for i in range(n)])


def around(value, axis, *held, cut=None):
    half = cut or value.shape[0] // 2
    left = shift(value, axis, 1)
    right = shift(value, axis, -1)
    left, right, *held = lax.optimization_barrier((left, right, *held))
    far_low = shift(left[:half], axis, 1)
    far_high = shift(right[half:], axis, -1)
    return value, left, right, far_low, far_high, *held


def copy_for_each(value, axis):
    n = lax.axis_size(axis)
    return lax.all_to_all(
        jnp.broadcast_to(value[None], (n, *value.shape)), axis, 0, 0, tiled=True
    )


def scatter_sum(own, to_right, to_left, keep_right, keep_left):
    half = own.shape[0] // 2
    from_left = shift(to_right, "tp_0", 1)
    from_right = shift(to_left, "tp_0", -1)
    add = lambda a, b: (a.astype(F32) + b.astype(F32)).astype(BF16)
    low = shift(add(keep_right, from_left[:half]), "tp_0", 1)
    high = shift(add(keep_left, from_right[:half]), "tp_0", -1)
    low, high, from_left, from_right = lax.optimization_barrier((low, high, from_left, from_right))
    top = own[:half].astype(F32) + from_right[half:].astype(F32) + low.astype(F32)
    bottom = own[half:].astype(F32) + from_left[half:].astype(F32) + high.astype(F32)
    return jnp.concatenate([top, bottom], axis=0).astype(BF16)


def put_pieces(j, half, block, own, to_right, to_left, keep_right, keep_left, rows):
    if j == 0:
        own[rows, :] = block
    elif j == 1:
        if half == 0:
            keep_right[...] = block
        else:
            to_right[rows, :] = block
    elif j == 2:
        if half == 0:
            to_right[: block.shape[0], :] = block
        else:
            to_left[: block.shape[0], :] = block
    else:
        if half == 0:
            to_left[block.shape[0] :, :] = block
        else:
            keep_left[...] = block


def dot_nt(a, b):
    return lax.dot_general(a, b, (((1,), (1,)), ((), ())), preferred_element_type=F32)


PARTS_Y = ((0, 0, 8), (3, 0, 8), (1, 0, 8), (2, 0, 4), (2, 4, 8))


def mixer_kernel(
    place, own, left, right, low, high, *rest
):
    pieces, rest = rest[:10], rest[10:]
    taps, gain, o_own, o_right, o_left, o_keep_right, o_keep_left = rest[:7]
    weights, normed, outer, signal, mixed, sems = rest[7:]
    x, k, y = place[0], place[1], place[2]
    copies = []
    for side in range(2):
        slot = k if side == 0 else 1 - k
        for q, (turn, begin, end) in enumerate(PARTS_Y):
            at = lax.rem(y + turn, 4)
            for b in range(begin, end):
                row = pl.multiple_of((b * 4 + at) * 64, 64)
                copies.append(
                    pltpu.make_async_copy(
                        pieces[side * 5 + q].at[b - begin],
                        weights.at[slot, pl.ds(row, 64), :],
                        sems.at[len(copies)],
                    )
                )
    for copy in copies:
        copy.start()
    half = normed.shape[0] // 2
    positions = [lax.rem(x + j, 4) for j in range(4)]
    for i, (begin, size, steps) in enumerate(((0, 96, 3), (288, 64, 4))):

        @pl.loop(0, steps)
        def _(tile):
            at = pl.multiple_of(tile * size, 32)
            r, h = pl.ds(begin + at, size), pl.ds(at, size)
            floats = [b.astype(F32) for b in (own[r, :], right[r, :], (low if i == 0 else high)[h, :], left[r, :])]
            squares = sum(jnp.sum(f * f, axis=1, keepdims=True) for f in floats)
            factor = lax.rsqrt(squares * (1.0 / 2048) + EPS)
            for j in range(4):
                g = gain[pl.ds(positions[j], 1), :]
                start = pl.multiple_of(positions[j] * 512, 512)
                normed[r, pl.ds(start, 512)] = (floats[j] * factor * g).astype(BF16)

    for copy in copies:
        copy.wait()
    signal[0:8, :] = jnp.zeros((8, 256), F32)

    @pl.loop(0, 2)
    def _(i):
        at = pl.multiple_of(i * half, 16)
        for c in range(2):
            ch = slice(c * 128, (c + 1) * 128)
            product = jnp.dot(normed[pl.ds(at, half), :], weights[c, :, 0:384], preferred_element_type=F32)
            outer[pl.ds(at, half), ch] = product[:, 0:128]
            signal[pl.ds(at + 8, half), ch] = product[:, 128:256] * product[:, 256:384]

    base = pl.multiple_of(k * HALO, HALO)

    @pl.loop(0, 2)
    def _(tile):
        at = pl.multiple_of(tile * 256, 256)
        for c in range(2):
            ch = slice(c * 128, (c + 1) * 128)
            s = signal[pl.ds(base + at, 264), ch]
            t = taps[:, ch]
            conv = t[0:1] * s[6:262] + t[1:2] * s[7:263] + t[2:3] * s[8:264]
            gated = outer[pl.ds(base + at, 256), ch] * conv
            scale = lax.rsqrt(jnp.mean(gated * gated, axis=1, keepdims=True) + EPS)
            mixed[pl.ds(at, 256), ch] = (gated * scale).astype(BF16)

    for j in range(4):
        start = pl.multiple_of(positions[j] * 512, 512)
        for zz in range(2):
            n = pl.ds(start + zz * 256, 256)
            w = jnp.concatenate([weights[0, n, 384:512], weights[1, n, 384:512]], axis=1)
            share = dot_nt(mixed[...], w).astype(BF16)
            cols = slice(zz * 256, (zz + 1) * 256)
            for h in range(2):
                put_pieces(
                    j, h, share[h * 256 : (h + 1) * 256],
                    *(ref.at[:, cols] for ref in (o_own, o_right, o_left, o_keep_right, o_keep_left)),
                    slice(h * 256, (h + 1) * 256),
                )


def norm_kernel(
    place, t_own, t_left, t_right, t_far, m_own, m_left, m_right, m_low, m_high,
    merge_gain, channel_gain, arrived, normed, o_first, near, sem,
):
    copy = pltpu.make_async_copy(arrived, near, sem)
    copy.start()
    x, k = place[0], place[1]
    positions = [lax.rem(x + j, 4) for j in range(4)]
    base = pl.multiple_of(k * HALO, HALO)
    for i in range(2):

        @pl.loop(0, 8)
        def _(tile):
            at = pl.multiple_of(tile * 32, 32)
            r, h = pl.ds(i * 256 + at, 32), pl.ds(at, 32)
            tr = pl.ds(base + i * 256 + at, 32)
            merged = [b.astype(F32) for b in (m_own[r, :], m_right[r, :], (m_low if i == 0 else m_high)[h, :], m_left[r, :])]
            toks = [b[tr, :].astype(F32) for b in (t_own, t_right, t_far, t_left)]
            squares = sum(jnp.sum(f * f, axis=1, keepdims=True) for f in merged)
            factor = lax.rsqrt(squares * (1.0 / 2048) + EPS)
            first = []
            for j in range(4):
                g = merge_gain[pl.ds(positions[j], 1), :]
                first.append((toks[j] + merged[j] * factor * g).astype(BF16))
            o_first[r, :] = first[0]
            first = [f.astype(F32) for f in first]
            squares = sum(jnp.sum(f * f, axis=1, keepdims=True) for f in first)
            factor = lax.rsqrt(squares * (1.0 / 2048) + EPS)
            for j in range(4):
                g = channel_gain[pl.ds(positions[j], 1), :]
                start = pl.multiple_of(positions[j] * 512, 512)
                normed[r, pl.ds(start, 512)] = (first[j] * factor * g).astype(BF16)

    copy.wait()


def pack_kernel(gate, up, down, out):
    out[:, 0:640] = gate[:, 0:640]
    out[:, 640:1280] = up[:, 0:640]
    out[:, 1280:1408] = jnp.concatenate([gate[:, 640:704], up[:, 640:704]], axis=1)
    out[:, 1408:2048] = down[:, 0:640]
    out[:, 2048:2176] = jnp.concatenate([down[:, 640:704], jnp.zeros((64, 64), BF16)], axis=1)


def forward_kernel(place, normed, weights, out):
    x = place[0]
    lane = lax.broadcasted_iota(jnp.int32, (256, 128), 1)

    @pl.loop(0, 2)
    def _(i):
        r = pl.ds(pl.multiple_of(i * 256, 256), 256)
        both = jnp.dot(normed[r, :], weights[:, 0:1408], preferred_element_type=F32)
        gate, up, tail = both[:, 0:640], both[:, 640:1280], both[:, 1280:1408]
        hidden = (gate / (1.0 + jnp.exp(-gate)) * up).astype(BF16)
        other = pltpu.roll(tail, 64, 1)
        last = jnp.where(lane < 64, tail / (1.0 + jnp.exp(-tail)) * other, 0.0)
        hidden = jnp.concatenate([hidden, last.astype(BF16)], axis=1)
        for j in range(4):
            start = pl.multiple_of(lax.rem(x + j, 4) * 512, 512)
            for zz in range(2):
                n = pl.ds(start + zz * 256, 256)
                out[j, r, zz * 256 : (zz + 1) * 256] = dot_nt(hidden, weights[n, 1408:2176]).astype(BF16)


VM = pl.BlockSpec(memory_space=pltpu.VMEM)
SM = pl.BlockSpec(memory_space=pltpu.SMEM)
HB = pl.BlockSpec(memory_space=pltpu.HBM)
SHARES = [
    jax.ShapeDtypeStruct((512, 512), BF16),
    jax.ShapeDtypeStruct((512, 512), BF16),
    jax.ShapeDtypeStruct((512, 512), BF16),
    jax.ShapeDtypeStruct((256, 512), BF16),
    jax.ShapeDtypeStruct((256, 512), BF16),
]


def shards(
    tokens, mixer_gain, conv_taps, outer_weight, inner_weight, value_weight, merge_weight,
    merge_gain, channel_gain, gate_weight, up_weight, down_weight, output_gain,
):
    x, k = lax.axis_index("tp_0"), lax.axis_index("tp_1")
    y = lax.axis_index("fs_1")
    place = jnp.stack([x, k, y]).astype(jnp.int32)
    span = 512 + HALO

    first_weights = jnp.concatenate([outer_weight, inner_weight, value_weight, merge_weight.T], axis=1)
    second_weights = pl.pallas_call(
        pack_kernel, out_shape=jax.ShapeDtypeStruct((64, 2176), BF16), in_specs=[VM] * 3, out_specs=VM
    )(gate_weight, up_weight, down_weight.T)
    second = lax.all_gather(second_weights, FS, axis=0, tiled=True)

    kept = lax.dynamic_slice_in_dim(tokens, k * (512 - HALO), span, 0)
    given = lax.dynamic_slice_in_dim(tokens, (1 - k) * (512 - HALO), span, 0)
    taken = shift(given, "tp_1", 1)
    block = jnp.where(k == 0, jnp.concatenate([kept, taken], 1), jnp.concatenate([taken, kept], 1))
    t_own, t_left, t_right, t_low, t_high = around(block, "tp_0", cut=288)

    plane = copy_for_each(first_weights, "fs_0")
    near = around(plane, "fs_1")
    near_other = [shift(part, "tp_1", 1) for part in near]

    own_taps = lax.dynamic_slice_in_dim(conv_taps, x * 256, 256, 1).astype(F32)
    pieces = pl.pallas_call(
        mixer_kernel,
        out_shape=SHARES,
        in_specs=[SM] + [VM] * 5 + [HB] * 10 + [VM] * 2,
        out_specs=[VM] * 5,
        scratch_shapes=[
            pltpu.VMEM((2, 2048, 512), BF16),
            pltpu.VMEM((span, 2048), BF16),
            pltpu.VMEM((span, 256), F32),
            pltpu.VMEM((span + 8, 256), F32),
            pltpu.VMEM((512, 256), BF16),
            pltpu.SemaphoreType.DMA((64,)),
        ],
        compiler_params=pltpu.CompilerParams(vmem_limit_bytes=26 * 2**20),
        cost_estimate=pl.CostEstimate(flops=2_300_000_000, bytes_accessed=9_000_000, transcendentals=0),
    )(place, t_own, t_left, t_right, t_low, t_high, *near, *near_other, own_taps, mixer_gain.reshape(4, 512))
    merged = scatter_sum(*pieces)
    *gathered, second = around(merged, "tp_0", second)

    normed, first, second = pl.pallas_call(
        norm_kernel,
        out_shape=[
            jax.ShapeDtypeStruct((512, 2048), BF16),
            jax.ShapeDtypeStruct((512, 512), BF16),
            jax.ShapeDtypeStruct((2048, 2176), BF16),
        ],
        in_specs=[SM] + [VM] * 11 + [HB],
        out_specs=[VM] * 3,
        scratch_shapes=[pltpu.SemaphoreType.DMA],
        compiler_params=pltpu.CompilerParams(vmem_limit_bytes=32 * 2**20),
        cost_estimate=pl.CostEstimate(flops=30_000_000, bytes_accessed=6_500_000, transcendentals=0),
    )(
        place, t_own, t_left, t_right, jnp.concatenate([t_low, t_high], 0), *gathered,
        merge_gain.reshape(4, 512), channel_gain.reshape(4, 512), second,
    )
    forward = pl.pallas_call(
        forward_kernel,
        out_shape=jax.ShapeDtypeStruct((4, 512, 512), BF16),
        in_specs=[SM] + [VM] * 2,
        out_specs=VM,
        compiler_params=pltpu.CompilerParams(vmem_limit_bytes=20 * 2**20),
        cost_estimate=pl.CostEstimate(flops=4_500_000_000, bytes_accessed=13_000_000, transcendentals=0),
    )
    theirs = shift(forward(place, shift(normed, "tp_1", 1), second), "tp_1", 1).astype(F32)
    ours = forward(place, normed, second).astype(F32) + theirs
    ours = ours.astype(BF16)
    pieces = (
        ours[0],
        jnp.concatenate([ours[2, :256], ours[1, 256:]], 0),
        jnp.concatenate([ours[2, 256:], ours[3, :256]], 0),
        ours[1, :256],
        ours[3, 256:],
    )
    down = scatter_sum(*pieces).astype(F32)
    squares = jnp.sum(down * down, axis=1).reshape(1, 4, 128)
    total = lax.all_to_all(jnp.broadcast_to(squares, (4, 4, 128)), "tp_0", 0, 0, tiled=True).sum(0)
    factor = lax.rsqrt(total.reshape(512, 1) / 2048 + EPS)
    own_gain = lax.dynamic_slice_in_dim(output_gain, x * 512, 512)
    result = (first.astype(F32) + down * factor * own_gain).astype(BF16)
    kept = lax.dynamic_slice_in_dim(result, k * 256, 256, 1)
    given = lax.dynamic_slice_in_dim(result, (1 - k) * 256, 256, 1)
    taken = shift(given, "tp_1", 1)
    return jnp.where(k == 0, jnp.concatenate([kept, taken], 0), jnp.concatenate([taken, kept], 0))


def solution(mesh):
    finer = Mesh(mesh.devices.reshape(8, 4, 4, 2), ("fs_0", "fs_1", "tp_0", "tp_1"))
    wide, tall = P(FS, TP), P(TP, FS)
    placed = (wide, P(), P(), wide, wide, wide, tall, P(), P(), wide, wide, tall, P())
    named = lambda *args: shards(*args)
    return jax.shard_map(named, mesh=finer, in_specs=placed, out_specs=P(FS, TP), check_vma=False)
```

```python
import jax
import jax.numpy as jnp
from jax import lax
from jax.experimental import pallas as pl
from jax.experimental.pallas import tpu as pltpu
from jax.sharding import Mesh
from jax.sharding import PartitionSpec as P

TP = ("tp_0", "tp_1")
FS = ("fs_0", "fs_1")
EPS = 1e-06
HALO = 32
F32 = jnp.float32
BF16 = jnp.bfloat16


def shift(value, axis, by):
    n = lax.axis_size(axis)
    return lax.ppermute(value, axis, [(i, (i + by) % n) for i in range(n)])


def around(value, axis, *held, cut=None):
    half = cut or value.shape[0] // 2
    left = shift(value, axis, 1)
    right = shift(value, axis, -1)
    left, right, *held = lax.optimization_barrier((left, right, *held))
    far_low = shift(left[:half], axis, 1)
    far_high = shift(right[half:], axis, -1)
    return value, left, right, far_low, far_high, *held


def copy_for_each(value, axis):
    n = lax.axis_size(axis)
    return lax.all_to_all(
        jnp.broadcast_to(value[None], (n, *value.shape)), axis, 0, 0, tiled=True
    )


def scatter_sum(own, to_right, to_left, keep_right, keep_left):
    half = own.shape[0] // 2
    from_left = shift(to_right, "tp_0", 1)
    from_right = shift(to_left, "tp_0", -1)
    add = lambda a, b: (a.astype(F32) + b.astype(F32)).astype(BF16)
    low = shift(add(keep_right, from_left[:half]), "tp_0", 1)
    high = shift(add(keep_left, from_right[:half]), "tp_0", -1)
    low, high, from_left, from_right = lax.optimization_barrier((low, high, from_left, from_right))
    top = own[:half].astype(F32) + from_right[half:].astype(F32) + low.astype(F32)
    bottom = own[half:].astype(F32) + from_left[half:].astype(F32) + high.astype(F32)
    return jnp.concatenate([top, bottom], axis=0).astype(BF16)


def put_pieces(j, half, block, own, to_right, to_left, keep_right, keep_left, rows):
    if j == 0:
        own[rows, :] = block
    elif j == 1:
        if half == 0:
            keep_right[...] = block
        else:
            to_right[rows, :] = block
    elif j == 2:
        if half == 0:
            to_right[: block.shape[0], :] = block
        else:
            to_left[: block.shape[0], :] = block
    else:
        if half == 0:
            to_left[block.shape[0] :, :] = block
        else:
            keep_left[...] = block


def dot_nt(a, b):
    return lax.dot_general(a, b, (((1,), (1,)), ((), ())), preferred_element_type=F32)


PARTS_Y = ((0, 0, 8), (3, 0, 8), (1, 0, 8), (2, 0, 4), (2, 4, 8))


def mixer_kernel(
    place, own, left, right, low, high, *rest
):
    pieces, rest = rest[:10], rest[10:]
    taps, gain, o_own, o_right, o_left, o_keep_right, o_keep_left = rest[:7]
    weights, normed, outer, signal, mixed, sems = rest[7:]
    x, k, y = place[0], place[1], place[2]
    copies = []
    for side in range(2):
        slot = k if side == 0 else 1 - k
        for q, (turn, begin, end) in enumerate(PARTS_Y):
            at = lax.rem(y + turn, 4)
            for b in range(begin, end):
                row = pl.multiple_of((b * 4 + at) * 64, 64)
                copies.append(
                    pltpu.make_async_copy(
                        pieces[side * 5 + q].at[b - begin],
                        weights.at[slot, pl.ds(row, 64), :],
                        sems.at[len(copies)],
                    )
                )
    for copy in copies:
        copy.start()
    half = normed.shape[0] // 2
    positions = [lax.rem(x + j, 4) for j in range(4)]
    for i, (begin, size, steps) in enumerate(((0, 96, 3), (288, 64, 4))):

        @pl.loop(0, steps)
        def _(tile):
            at = pl.multiple_of(tile * size, 32)
            r, h = pl.ds(begin + at, size), pl.ds(at, size)
            floats = [b.astype(F32) for b in (own[r, :], right[r, :], (low if i == 0 else high)[h, :], left[r, :])]
            squares = sum(jnp.sum(f * f, axis=1, keepdims=True) for f in floats)
            factor = lax.rsqrt(squares * (1.0 / 2048) + EPS)
            for j in range(4):
                g = gain[pl.ds(positions[j], 1), :]
                start = pl.multiple_of(positions[j] * 512, 512)
                normed[r, pl.ds(start, 512)] = (floats[j] * factor * g).astype(BF16)

    for copy in copies:
        copy.wait()
    signal[0:8, :] = jnp.zeros((8, 256), F32)

    @pl.loop(0, 2)
    def _(i):
        at = pl.multiple_of(i * half, 16)
        for c in range(2):
            ch = slice(c * 128, (c + 1) * 128)
            product = jnp.dot(normed[pl.ds(at, half), :], weights[c, :, 0:384], preferred_element_type=F32)
            outer[pl.ds(at, half), ch] = product[:, 0:128]
            signal[pl.ds(at + 8, half), ch] = product[:, 128:256] * product[:, 256:384]

    base = pl.multiple_of(k * HALO, HALO)

    @pl.loop(0, 2)
    def _(tile):
        at = pl.multiple_of(tile * 256, 256)
        for c in range(2):
            ch = slice(c * 128, (c + 1) * 128)
            s = signal[pl.ds(base + at, 264), ch]
            t = taps[:, ch]
            conv = t[0:1] * s[6:262] + t[1:2] * s[7:263] + t[2:3] * s[8:264]
            gated = outer[pl.ds(base + at, 256), ch] * conv
            scale = lax.rsqrt(jnp.mean(gated * gated, axis=1, keepdims=True) + EPS)
            mixed[pl.ds(at, 256), ch] = (gated * scale).astype(BF16)

    for j in range(4):
        start = pl.multiple_of(positions[j] * 512, 512)
        for zz in range(2):
            n = pl.ds(start + zz * 256, 256)
            w = jnp.concatenate([weights[0, n, 384:512], weights[1, n, 384:512]], axis=1)
            share = dot_nt(mixed[...], w).astype(BF16)
            cols = slice(zz * 256, (zz + 1) * 256)
            for h in range(2):
                put_pieces(
                    j, h, share[h * 256 : (h + 1) * 256],
                    *(ref.at[:, cols] for ref in (o_own, o_right, o_left, o_keep_right, o_keep_left)),
                    slice(h * 256, (h + 1) * 256),
                )


def norm_kernel(
    place, t_own, t_left, t_right, t_far, m_own, m_left, m_right, m_low, m_high,
    merge_gain, channel_gain, arrived, normed, o_first, near, sem,
):
    copy = pltpu.make_async_copy(arrived, near, sem)
    copy.start()
    x, k = place[0], place[1]
    positions = [lax.rem(x + j, 4) for j in range(4)]
    base = pl.multiple_of(k * HALO, HALO)
    for i in range(2):

        @pl.loop(0, 8)
        def _(tile):
            at = pl.multiple_of(tile * 32, 32)
            r, h = pl.ds(i * 256 + at, 32), pl.ds(at, 32)
            tr = pl.ds(base + i * 256 + at, 32)
            merged = [b.astype(F32) for b in (m_own[r, :], m_right[r, :], (m_low if i == 0 else m_high)[h, :], m_left[r, :])]
            toks = [b[tr, :].astype(F32) for b in (t_own, t_right, t_far, t_left)]
            squares = sum(jnp.sum(f * f, axis=1, keepdims=True) for f in merged)
            factor = lax.rsqrt(squares * (1.0 / 2048) + EPS)
            first = []
            for j in range(4):
                g = merge_gain[pl.ds(positions[j], 1), :]
                first.append((toks[j] + merged[j] * factor * g).astype(BF16))
            o_first[r, :] = first[0]
            first = [f.astype(F32) for f in first]
            squares = sum(jnp.sum(f * f, axis=1, keepdims=True) for f in first)
            factor = lax.rsqrt(squares * (1.0 / 2048) + EPS)
            for j in range(4):
                g = channel_gain[pl.ds(positions[j], 1), :]
                start = pl.multiple_of(positions[j] * 512, 512)
                normed[r, pl.ds(start, 512)] = (first[j] * factor * g).astype(BF16)

    copy.wait()


def pack_kernel(gate, up, down, out):
    out[:, 0:640] = gate[:, 0:640]
    out[:, 640:1280] = up[:, 0:640]
    out[:, 1280:1408] = jnp.concatenate([gate[:, 640:704], up[:, 640:704]], axis=1)
    out[:, 1408:2048] = down[:, 0:640]
    out[:, 2048:2176] = jnp.concatenate([down[:, 640:704], jnp.zeros((64, 64), BF16)], axis=1)


def forward_kernel(place, normed, mine, other, out, fetched, hidden, sem):
    copy = pltpu.make_async_copy(other, fetched, sem)
    copy.start()
    x = place[0]
    lane = lax.broadcasted_iota(jnp.int32, (256, 128), 1)
    for c, weights in enumerate((mine, fetched)):
        if c == 1:
            copy.wait()

        @pl.loop(0, 2)
        def _(i):
            r = pl.ds(pl.multiple_of(i * 256, 256), 256)
            both = jnp.dot(normed[r, :], weights[:, 0:1408], preferred_element_type=F32)
            gate, up, tail = both[:, 0:640], both[:, 640:1280], both[:, 1280:1408]
            hidden[r, c * 768 : c * 768 + 640] = (gate / (1.0 + jnp.exp(-gate)) * up).astype(BF16)
            last = tail / (1.0 + jnp.exp(-tail)) * pltpu.roll(tail, 64, 1)
            hidden[r, c * 768 + 640 : (c + 1) * 768] = jnp.where(lane < 64, last, 0.0).astype(BF16)

    @pl.loop(0, 2)
    def _(i):
        r = pl.ds(pl.multiple_of(i * 256, 256), 256)
        for j in range(4):
            start = pl.multiple_of(lax.rem(x + j, 4) * 512, 512)
            for zz in range(2):
                n = pl.ds(start + zz * 256, 256)
                share = dot_nt(hidden[r, 0:768], mine[n, 1408:2176])
                share += dot_nt(hidden[r, 768:1536], fetched[n, 1408:2176])
                out[j, r, zz * 256 : (zz + 1) * 256] = share.astype(BF16)


VM = pl.BlockSpec(memory_space=pltpu.VMEM)
SM = pl.BlockSpec(memory_space=pltpu.SMEM)
HB = pl.BlockSpec(memory_space=pltpu.HBM)
SHARES = [
    jax.ShapeDtypeStruct((512, 512), BF16),
    jax.ShapeDtypeStruct((512, 512), BF16),
    jax.ShapeDtypeStruct((512, 512), BF16),
    jax.ShapeDtypeStruct((256, 512), BF16),
    jax.ShapeDtypeStruct((256, 512), BF16),
]


def shards(
    tokens, mixer_gain, conv_taps, outer_weight, inner_weight, value_weight, merge_weight,
    merge_gain, channel_gain, gate_weight, up_weight, down_weight, output_gain,
):
    x, k = lax.axis_index("tp_0"), lax.axis_index("tp_1")
    y = lax.axis_index("fs_1")
    place = jnp.stack([x, k, y]).astype(jnp.int32)
    span = 512 + HALO

    first_weights = jnp.concatenate([outer_weight, inner_weight, value_weight, merge_weight.T], axis=1)
    second_weights = pl.pallas_call(
        pack_kernel, out_shape=jax.ShapeDtypeStruct((64, 2176), BF16), in_specs=[VM] * 3, out_specs=VM
    )(gate_weight, up_weight, down_weight.T)
    second = lax.all_gather(second_weights, FS, axis=0, tiled=True)

    kept = lax.dynamic_slice_in_dim(tokens, k * (512 - HALO), span, 0)
    given = lax.dynamic_slice_in_dim(tokens, (1 - k) * (512 - HALO), span, 0)
    taken = shift(given, "tp_1", 1)
    block = jnp.where(k == 0, jnp.concatenate([kept, taken], 1), jnp.concatenate([taken, kept], 1))
    t_own, t_left, t_right, t_low, t_high = around(block, "tp_0", cut=288)

    plane = copy_for_each(first_weights, "fs_0")
    near = around(plane, "fs_1")
    near_other = [shift(part, "tp_1", 1) for part in near]

    own_taps = lax.dynamic_slice_in_dim(conv_taps, x * 256, 256, 1).astype(F32)
    pieces = pl.pallas_call(
        mixer_kernel,
        out_shape=SHARES,
        in_specs=[SM] + [VM] * 5 + [HB] * 10 + [VM] * 2,
        out_specs=[VM] * 5,
        scratch_shapes=[
            pltpu.VMEM((2, 2048, 512), BF16),
            pltpu.VMEM((span, 2048), BF16),
            pltpu.VMEM((span, 256), F32),
            pltpu.VMEM((span + 8, 256), F32),
            pltpu.VMEM((512, 256), BF16),
            pltpu.SemaphoreType.DMA((64,)),
        ],
        compiler_params=pltpu.CompilerParams(vmem_limit_bytes=26 * 2**20),
        cost_estimate=pl.CostEstimate(flops=2_300_000_000, bytes_accessed=9_000_000, transcendentals=0),
    )(place, t_own, t_left, t_right, t_low, t_high, *near, *near_other, own_taps, mixer_gain.reshape(4, 512))
    merged = scatter_sum(*pieces)
    second_other = shift(second, "tp_1", 1)
    *gathered, second = around(merged, "tp_0", second)

    normed, first, second = pl.pallas_call(
        norm_kernel,
        out_shape=[
            jax.ShapeDtypeStruct((512, 2048), BF16),
            jax.ShapeDtypeStruct((512, 512), BF16),
            jax.ShapeDtypeStruct((2048, 2176), BF16),
        ],
        in_specs=[SM] + [VM] * 11 + [HB],
        out_specs=[VM] * 3,
        scratch_shapes=[pltpu.SemaphoreType.DMA],
        compiler_params=pltpu.CompilerParams(vmem_limit_bytes=32 * 2**20),
        cost_estimate=pl.CostEstimate(flops=30_000_000, bytes_accessed=6_500_000, transcendentals=0),
    )(
        place, t_own, t_left, t_right, jnp.concatenate([t_low, t_high], 0), *gathered,
        merge_gain.reshape(4, 512), channel_gain.reshape(4, 512), second,
    )
    ours = pl.pallas_call(
        forward_kernel,
        out_shape=jax.ShapeDtypeStruct((4, 512, 512), BF16),
        in_specs=[SM] + [VM] * 2 + [HB],
        out_specs=VM,
        scratch_shapes=[
            pltpu.VMEM((2048, 2176), BF16),
            pltpu.VMEM((512, 1536), BF16),
            pltpu.SemaphoreType.DMA,
        ],
        compiler_params=pltpu.CompilerParams(vmem_limit_bytes=34 * 2**20),
        cost_estimate=pl.CostEstimate(flops=9_000_000_000, bytes_accessed=13_000_000, transcendentals=0),
    )(place, normed, second, second_other)
    pieces = (
        ours[0],
        jnp.concatenate([ours[2, :256], ours[1, 256:]], 0),
        jnp.concatenate([ours[2, 256:], ours[3, :256]], 0),
        ours[1, :256],
        ours[3, 256:],
    )
    down = scatter_sum(*pieces).astype(F32)
    squares = jnp.sum(down * down, axis=1).reshape(1, 4, 128)
    total = lax.all_to_all(jnp.broadcast_to(squares, (4, 4, 128)), "tp_0", 0, 0, tiled=True).sum(0)
    factor = lax.rsqrt(total.reshape(512, 1) / 2048 + EPS)
    own_gain = lax.dynamic_slice_in_dim(output_gain, x * 512, 512)
    result = (first.astype(F32) + down * factor * own_gain).astype(BF16)
    kept = lax.dynamic_slice_in_dim(result, k * 256, 256, 1)
    given = lax.dynamic_slice_in_dim(result, (1 - k) * 256, 256, 1)
    taken = shift(given, "tp_1", 1)
    return jnp.where(k == 0, jnp.concatenate([kept, taken], 0), jnp.concatenate([taken, kept], 0))


def solution(mesh):
    finer = Mesh(mesh.devices.reshape(8, 4, 4, 2), ("fs_0", "fs_1", "tp_0", "tp_1"))
    wide, tall = P(FS, TP), P(TP, FS)
    placed = (wide, P(), P(), wide, wide, wide, tall, P(), P(), wide, wide, tall, P())
    named = lambda *args: shards(*args)
    return jax.shard_map(named, mesh=finer, in_specs=placed, out_specs=P(FS, TP), check_vma=False)
```

```python
import jax
import jax.numpy as jnp
from jax import lax
from jax.experimental import pallas as pl
from jax.experimental.pallas import tpu as pltpu
from jax.sharding import Mesh
from jax.sharding import PartitionSpec as P

TP = ("tp_0", "tp_1")
FS = ("fs_0", "fs_1")
EPS = 1e-06
HALO = 32
F32 = jnp.float32
BF16 = jnp.bfloat16


def shift(value, axis, by):
    n = lax.axis_size(axis)
    return lax.ppermute(value, axis, [(i, (i + by) % n) for i in range(n)])


def around(value, axis, *held, cut=None):
    half = cut or value.shape[0] // 2
    left = shift(value, axis, 1)
    right = shift(value, axis, -1)
    left, right, *held = lax.optimization_barrier((left, right, *held))
    far_low = shift(left[:half], axis, 1)
    far_high = shift(right[half:], axis, -1)
    return value, left, right, far_low, far_high, *held


def copy_for_each(value, axis):
    n = lax.axis_size(axis)
    return lax.all_to_all(
        jnp.broadcast_to(value[None], (n, *value.shape)), axis, 0, 0, tiled=True
    )


def scatter_sum(own, to_right, to_left, keep_right, keep_left):
    half = own.shape[0] // 2
    from_left = shift(to_right, "tp_0", 1)
    from_right = shift(to_left, "tp_0", -1)
    add = lambda a, b: (a.astype(F32) + b.astype(F32)).astype(BF16)
    low = shift(add(keep_right, from_left[:half]), "tp_0", 1)
    high = shift(add(keep_left, from_right[:half]), "tp_0", -1)
    low, high, from_left, from_right = lax.optimization_barrier((low, high, from_left, from_right))
    top = own[:half].astype(F32) + from_right[half:].astype(F32) + low.astype(F32)
    bottom = own[half:].astype(F32) + from_left[half:].astype(F32) + high.astype(F32)
    return jnp.concatenate([top, bottom], axis=0).astype(BF16)


def put_pieces(j, half, block, own, to_right, to_left, keep_right, keep_left, rows):
    if j == 0:
        own[rows, :] = block
    elif j == 1:
        if half == 0:
            keep_right[...] = block
        else:
            to_right[rows, :] = block
    elif j == 2:
        if half == 0:
            to_right[: block.shape[0], :] = block
        else:
            to_left[: block.shape[0], :] = block
    else:
        if half == 0:
            to_left[block.shape[0] :, :] = block
        else:
            keep_left[...] = block


def dot_nt(a, b):
    return lax.dot_general(a, b, (((1,), (1,)), ((), ())), preferred_element_type=F32)


PARTS_Y = ((0, 0, 8), (3, 0, 8), (1, 0, 8), (2, 0, 4), (2, 4, 8))


def mixer_kernel(
    place, own, left, right, low, high, *rest
):
    pieces, rest = rest[:10], rest[10:]
    taps, gain, o_own, o_right, o_left, o_keep_right, o_keep_left = rest[:7]
    weights, normed, outer, signal, mixed, sems = rest[7:]
    x, k, y = place[0], place[1], place[2]
    copies = []
    for side in range(2):
        slot = k if side == 0 else 1 - k
        for q, (turn, begin, end) in enumerate(PARTS_Y):
            target = weights.at[slot, begin:end, lax.rem(y + turn, 4)]
            copies.append(pltpu.make_async_copy(pieces[side * 5 + q], target, sems.at[len(copies)]))
    for copy in copies:
        copy.start()
    half = normed.shape[0] // 2
    positions = [lax.rem(x + j, 4) for j in range(4)]
    for i, (begin, size, steps) in enumerate(((0, 96, 3), (288, 64, 4))):

        @pl.loop(0, steps)
        def _(tile):
            at = pl.multiple_of(tile * size, 32)
            r, h = pl.ds(begin + at, size), pl.ds(at, size)
            floats = [b.astype(F32) for b in (own[r, :], right[r, :], (low if i == 0 else high)[h, :], left[r, :])]
            squares = sum(jnp.sum(f * f, axis=1, keepdims=True) for f in floats)
            factor = lax.rsqrt(squares * (1.0 / 2048) + EPS)
            for j in range(4):
                g = gain[pl.ds(positions[j], 1), :]
                start = pl.multiple_of(positions[j] * 512, 512)
                normed[r, pl.ds(start, 512)] = (floats[j] * factor * g).astype(BF16)

    for copy in copies:
        copy.wait()
    signal[0:8, :] = jnp.zeros((8, 256), F32)

    @pl.loop(0, 2)
    def _(i):
        at = pl.multiple_of(i * half, 16)
        for c in range(2):
            ch = slice(c * 128, (c + 1) * 128)
            product = jnp.dot(normed[pl.ds(at, half), :], weights[c, :, :, :, 0:384].reshape(2048, 384), preferred_element_type=F32)
            outer[pl.ds(at, half), ch] = product[:, 0:128]
            signal[pl.ds(at + 8, half), ch] = product[:, 128:256] * product[:, 256:384]

    base = pl.multiple_of(k * HALO, HALO)

    @pl.loop(0, 2)
    def _(tile):
        at = pl.multiple_of(tile * 256, 256)
        for c in range(2):
            ch = slice(c * 128, (c + 1) * 128)
            s = signal[pl.ds(base + at, 264), ch]
            t = taps[:, ch]
            conv = t[0:1] * s[6:262] + t[1:2] * s[7:263] + t[2:3] * s[8:264]
            gated = outer[pl.ds(base + at, 256), ch] * conv
            scale = lax.rsqrt(jnp.mean(gated * gated, axis=1, keepdims=True) + EPS)
            mixed[pl.ds(at, 256), ch] = (gated * scale).astype(BF16)

    for j in range(4):
        start = pl.multiple_of(positions[j] * 512, 512)
        for zz in range(2):
            n = 2 * positions[j] + zz
            w = [weights[c, n, :, :, 384:512].reshape(256, 128) for c in range(2)]
            w = jnp.concatenate(w, axis=1)
            share = dot_nt(mixed[...], w).astype(BF16)
            cols = slice(zz * 256, (zz + 1) * 256)
            for h in range(2):
                put_pieces(
                    j, h, share[h * 256 : (h + 1) * 256],
                    *(ref.at[:, cols] for ref in (o_own, o_right, o_left, o_keep_right, o_keep_left)),
                    slice(h * 256, (h + 1) * 256),
                )


def norm_kernel(
    place, t_own, t_left, t_right, t_far, m_own, m_left, m_right, m_low, m_high,
    merge_gain, channel_gain, arrived, normed, o_first, near, sem,
):
    copy = pltpu.make_async_copy(arrived, near, sem)
    copy.start()
    x, k = place[0], place[1]
    positions = [lax.rem(x + j, 4) for j in range(4)]
    base = pl.multiple_of(k * HALO, HALO)
    for i in range(2):

        @pl.loop(0, 4)
        def _(tile):
            at = pl.multiple_of(tile * 64, 64)
            r, h = pl.ds(i * 256 + at, 64), pl.ds(at, 64)
            tr = pl.ds(base + i * 256 + at, 64)
            merged = [b.astype(F32) for b in (m_own[r, :], m_right[r, :], (m_low if i == 0 else m_high)[h, :], m_left[r, :])]
            toks = [b[tr, :].astype(F32) for b in (t_own, t_right, t_far, t_left)]
            squares = sum(jnp.sum(f * f, axis=1, keepdims=True) for f in merged)
            factor = lax.rsqrt(squares * (1.0 / 2048) + EPS)
            first = []
            for j in range(4):
                g = merge_gain[pl.ds(positions[j], 1), :]
                first.append((toks[j] + merged[j] * factor * g).astype(BF16))
            o_first[r, :] = first[0]
            first = [f.astype(F32) for f in first]
            squares = sum(jnp.sum(f * f, axis=1, keepdims=True) for f in first)
            factor = lax.rsqrt(squares * (1.0 / 2048) + EPS)
            for j in range(4):
                g = channel_gain[pl.ds(positions[j], 1), :]
                start = pl.multiple_of(positions[j] * 512, 512)
                normed[r, pl.ds(start, 512)] = (first[j] * factor * g).astype(BF16)

    copy.wait()


def pack_kernel(gate, up, down, out):
    out[:, 0:640] = gate[:, 0:640]
    out[:, 640:1280] = up[:, 0:640]
    out[:, 1280:1408] = jnp.concatenate([gate[:, 640:704], up[:, 640:704]], axis=1)
    out[:, 1408:2048] = down[:, 0:640]
    out[:, 2048:2176] = jnp.concatenate([down[:, 640:704], jnp.zeros((64, 64), BF16)], axis=1)


def forward_kernel(place, normed, mine, other, out, fetched, hidden, sem):
    copy = pltpu.make_async_copy(other, fetched, sem)
    copy.start()
    x = place[0]
    lane = lax.broadcasted_iota(jnp.int32, (256, 128), 1)
    for c, weights in enumerate((mine, fetched)):
        if c == 1:
            copy.wait()

        @pl.loop(0, 2)
        def _(i):
            r = pl.ds(pl.multiple_of(i * 256, 256), 256)
            both = jnp.dot(normed[r, :], weights[:, 0:1408], preferred_element_type=F32)
            gate, up, tail = both[:, 0:640], both[:, 640:1280], both[:, 1280:1408]
            hidden[r, c * 768 : c * 768 + 640] = (gate / (1.0 + jnp.exp(-gate)) * up).astype(BF16)
            last = tail / (1.0 + jnp.exp(-tail)) * pltpu.roll(tail, 64, 1)
            hidden[r, c * 768 + 640 : (c + 1) * 768] = jnp.where(lane < 64, last, 0.0).astype(BF16)

    @pl.loop(0, 2)
    def _(i):
        r = pl.ds(pl.multiple_of(i * 256, 256), 256)
        for j in range(4):
            start = pl.multiple_of(lax.rem(x + j, 4) * 512, 512)
            for zz in range(2):
                n = pl.ds(start + zz * 256, 256)
                share = dot_nt(hidden[r, 0:768], mine[n, 1408:2176])
                share += dot_nt(hidden[r, 768:1536], fetched[n, 1408:2176])
                out[j, r, zz * 256 : (zz + 1) * 256] = share.astype(BF16)


VM = pl.BlockSpec(memory_space=pltpu.VMEM)
SM = pl.BlockSpec(memory_space=pltpu.SMEM)
HB = pl.BlockSpec(memory_space=pltpu.HBM)
SHARES = [
    jax.ShapeDtypeStruct((512, 512), BF16),
    jax.ShapeDtypeStruct((512, 512), BF16),
    jax.ShapeDtypeStruct((512, 512), BF16),
    jax.ShapeDtypeStruct((256, 512), BF16),
    jax.ShapeDtypeStruct((256, 512), BF16),
]


def shards(
    tokens, mixer_gain, conv_taps, outer_weight, inner_weight, value_weight, merge_weight,
    merge_gain, channel_gain, gate_weight, up_weight, down_weight, output_gain,
):
    x, k = lax.axis_index("tp_0"), lax.axis_index("tp_1")
    y = lax.axis_index("fs_1")
    place = jnp.stack([x, k, y]).astype(jnp.int32)
    span = 512 + HALO

    first_weights = jnp.concatenate([outer_weight, inner_weight, value_weight, merge_weight.T], axis=1)
    second_weights = pl.pallas_call(
        pack_kernel, out_shape=jax.ShapeDtypeStruct((64, 2176), BF16), in_specs=[VM] * 3, out_specs=VM
    )(gate_weight, up_weight, down_weight.T)
    second = lax.all_gather(second_weights, FS, axis=0, tiled=True)

    kept = lax.dynamic_slice_in_dim(tokens, k * (512 - HALO), span, 0)
    given = lax.dynamic_slice_in_dim(tokens, (1 - k) * (512 - HALO), span, 0)
    taken = shift(given, "tp_1", 1)
    block = jnp.where(k == 0, jnp.concatenate([kept, taken], 1), jnp.concatenate([taken, kept], 1))
    t_own, t_left, t_right, t_low, t_high = around(block, "tp_0", cut=288)

    plane = copy_for_each(first_weights, "fs_0")
    near = around(plane, "fs_1")
    near_other = [shift(part, "tp_1", 1) for part in near]

    own_taps = lax.dynamic_slice_in_dim(conv_taps, x * 256, 256, 1).astype(F32)
    pieces = pl.pallas_call(
        mixer_kernel,
        out_shape=SHARES,
        in_specs=[SM] + [VM] * 5 + [HB] * 10 + [VM] * 2,
        out_specs=[VM] * 5,
        scratch_shapes=[
            pltpu.VMEM((2, 8, 4, 64, 512), BF16),
            pltpu.VMEM((span, 2048), BF16),
            pltpu.VMEM((span, 256), F32),
            pltpu.VMEM((span + 8, 256), F32),
            pltpu.VMEM((512, 256), BF16),
            pltpu.SemaphoreType.DMA((10,)),
        ],
        compiler_params=pltpu.CompilerParams(vmem_limit_bytes=26 * 2**20),
        cost_estimate=pl.CostEstimate(flops=2_300_000_000, bytes_accessed=9_000_000, transcendentals=0),
    )(place, t_own, t_left, t_right, t_low, t_high, *near, *near_other, own_taps, mixer_gain.reshape(4, 512))
    merged = scatter_sum(*pieces)
    second_other = shift(second, "tp_1", 1)
    *gathered, second = around(merged, "tp_0", second)

    normed, first, second = pl.pallas_call(
        norm_kernel,
        out_shape=[
            jax.ShapeDtypeStruct((512, 2048), BF16),
            jax.ShapeDtypeStruct((512, 512), BF16),
            jax.ShapeDtypeStruct((2048, 2176), BF16),
        ],
        in_specs=[SM] + [VM] * 11 + [HB],
        out_specs=[VM] * 3,
        scratch_shapes=[pltpu.SemaphoreType.DMA],
        compiler_params=pltpu.CompilerParams(vmem_limit_bytes=32 * 2**20),
        cost_estimate=pl.CostEstimate(flops=30_000_000, bytes_accessed=6_500_000, transcendentals=0),
    )(
        place, t_own, t_left, t_right, jnp.concatenate([t_low, t_high], 0), *gathered,
        merge_gain.reshape(4, 512), channel_gain.reshape(4, 512), second,
    )
    ours = pl.pallas_call(
        forward_kernel,
        out_shape=jax.ShapeDtypeStruct((4, 512, 512), BF16),
        in_specs=[SM] + [VM] * 2 + [HB],
        out_specs=VM,
        scratch_shapes=[
            pltpu.VMEM((2048, 2176), BF16),
            pltpu.VMEM((512, 1536), BF16),
            pltpu.SemaphoreType.DMA,
        ],
        compiler_params=pltpu.CompilerParams(vmem_limit_bytes=34 * 2**20),
        cost_estimate=pl.CostEstimate(flops=9_000_000_000, bytes_accessed=13_000_000, transcendentals=0),
    )(place, normed, second, second_other)
    pieces = (
        ours[0],
        jnp.concatenate([ours[2, :256], ours[1, 256:]], 0),
        jnp.concatenate([ours[2, 256:], ours[3, :256]], 0),
        ours[1, :256],
        ours[3, 256:],
    )
    down = scatter_sum(*pieces).astype(F32)
    squares = jnp.sum(down * down, axis=1).reshape(4, 128)
    total = squares + shift(squares, "tp_0", 1) + shift(squares, "tp_0", -1) + shift(squares, "tp_0", 2)
    factor = lax.rsqrt(total.reshape(512, 1) / 2048 + EPS)
    own_gain = lax.dynamic_slice_in_dim(output_gain, x * 512, 512)
    result = (first.astype(F32) + down * factor * own_gain).astype(BF16)
    kept = lax.dynamic_slice_in_dim(result, k * 256, 256, 1)
    given = lax.dynamic_slice_in_dim(result, (1 - k) * 256, 256, 1)
    taken = shift(given, "tp_1", 1)
    return jnp.where(k == 0, jnp.concatenate([kept, taken], 0), jnp.concatenate([taken, kept], 0))


def solution(mesh):
    finer = Mesh(mesh.devices.reshape(8, 4, 4, 2), ("fs_0", "fs_1", "tp_0", "tp_1"))
    wide, tall = P(FS, TP), P(TP, FS)
    placed = (wide, P(), P(), wide, wide, wide, tall, P(), P(), wide, wide, tall, P())
    named = lambda *args: shards(*args)
    return jax.shard_map(named, mesh=finer, in_specs=placed, out_specs=P(FS, TP), check_vma=False)
```

```python
import jax
import jax.numpy as jnp
from jax import lax
from jax.experimental import pallas as pl
from jax.experimental.pallas import tpu as pltpu
from jax.sharding import Mesh
from jax.sharding import PartitionSpec as P

TP = ("tp_0", "tp_1")
FS = ("fs_0", "fs_1")
EPS = 1e-06
HALO = 32
F32 = jnp.float32
BF16 = jnp.bfloat16


def shift(value, axis, by):
    n = lax.axis_size(axis)
    return lax.ppermute(value, axis, [(i, (i + by) % n) for i in range(n)])


def around(value, axis, *held, cut=None):
    half = cut or value.shape[0] // 2
    left = shift(value, axis, 1)
    right = shift(value, axis, -1)
    if held:
        left, right, *held = lax.optimization_barrier((left, right, *held))
    far_low = shift(left[:half], axis, 1)
    far_high = shift(right[half:], axis, -1)
    return value, left, right, far_low, far_high, *held


def copy_for_each(value, axis):
    n = lax.axis_size(axis)
    return lax.all_to_all(
        jnp.broadcast_to(value[None], (n, *value.shape)), axis, 0, 0, tiled=True
    )


def scatter_sum(own, to_right, to_left, keep_right, keep_left):
    half = own.shape[0] // 2
    from_left = shift(to_right, "tp_0", 1)
    from_right = shift(to_left, "tp_0", -1)
    add = lambda a, b: (a.astype(F32) + b.astype(F32)).astype(BF16)
    low = shift(add(keep_right, from_left[:half]), "tp_0", 1)
    high = shift(add(keep_left, from_right[:half]), "tp_0", -1)
    low, high, from_left, from_right = lax.optimization_barrier((low, high, from_left, from_right))
    top = own[:half].astype(F32) + from_right[half:].astype(F32) + low.astype(F32)
    bottom = own[half:].astype(F32) + from_left[half:].astype(F32) + high.astype(F32)
    return jnp.concatenate([top, bottom], axis=0).astype(BF16)


def put_pieces(j, half, block, own, to_right, to_left, keep_right, keep_left, rows):
    if j == 0:
        own[rows, :] = block
    elif j == 1:
        if half == 0:
            keep_right[...] = block
        else:
            to_right[rows, :] = block
    elif j == 2:
        if half == 0:
            to_right[: block.shape[0], :] = block
        else:
            to_left[: block.shape[0], :] = block
    else:
        if half == 0:
            to_left[block.shape[0] :, :] = block
        else:
            keep_left[...] = block


def dot_nt(a, b):
    return lax.dot_general(a, b, (((1,), (1,)), ((), ())), preferred_element_type=F32)


PARTS_Y = ((0, 0, 8), (3, 0, 8), (1, 0, 8), (2, 0, 4), (2, 4, 8))


def mixer_kernel(
    place, own, left, right, low, high, *rest
):
    pieces, rest = rest[:10], rest[10:]
    taps, gain, o_own, o_right, o_left, o_keep_right, o_keep_left = rest[:7]
    weights, normed, outer, signal, mixed, sems = rest[7:]
    x, k, y = place[0], place[1], place[2]
    copies = []
    for side in range(2):
        slot = k if side == 0 else 1 - k
        for q, (turn, begin, end) in enumerate(PARTS_Y):
            target = weights.at[slot, begin:end, lax.rem(y + turn, 4)]
            copies.append(pltpu.make_async_copy(pieces[side * 5 + q], target, sems.at[len(copies)]))
    for copy in copies:
        copy.start()
    half = normed.shape[0] // 2
    positions = [lax.rem(x + j, 4) for j in range(4)]
    for i, (begin, size, steps) in enumerate(((0, 96, 3), (288, 64, 4))):

        @pl.loop(0, steps)
        def _(tile):
            at = pl.multiple_of(tile * size, 32)
            r, h = pl.ds(begin + at, size), pl.ds(at, size)
            floats = [b.astype(F32) for b in (own[r, :], right[r, :], (low if i == 0 else high)[h, :], left[r, :])]
            squares = sum(jnp.sum(f * f, axis=1, keepdims=True) for f in floats)
            factor = lax.rsqrt(squares * (1.0 / 2048) + EPS)
            for j in range(4):
                g = gain[pl.ds(positions[j], 1), :]
                start = pl.multiple_of(positions[j] * 512, 512)
                normed[r, pl.ds(start, 512)] = (floats[j] * factor * g).astype(BF16)

    for copy in copies:
        copy.wait()
    signal[0:8, :] = jnp.zeros((8, 256), F32)

    @pl.loop(0, 2)
    def _(i):
        at = pl.multiple_of(i * half, 16)
        for c in range(2):
            ch = slice(c * 128, (c + 1) * 128)
            product = jnp.dot(normed[pl.ds(at, half), :], weights[c, :, :, :, 0:384].reshape(2048, 384), preferred_element_type=F32)
            outer[pl.ds(at, half), ch] = product[:, 0:128]
            signal[pl.ds(at + 8, half), ch] = product[:, 128:256] * product[:, 256:384]

    base = pl.multiple_of(k * HALO, HALO)

    @pl.loop(0, 2)
    def _(tile):
        at = pl.multiple_of(tile * 256, 256)
        for c in range(2):
            ch = slice(c * 128, (c + 1) * 128)
            s = signal[pl.ds(base + at, 264), ch]
            t = taps[:, ch]
            conv = t[0:1] * s[6:262] + t[1:2] * s[7:263] + t[2:3] * s[8:264]
            gated = outer[pl.ds(base + at, 256), ch] * conv
            scale = lax.rsqrt(jnp.mean(gated * gated, axis=1, keepdims=True) + EPS)
            mixed[pl.ds(at, 256), ch] = (gated * scale).astype(BF16)

    for j in range(4):
        start = pl.multiple_of(positions[j] * 512, 512)
        for zz in range(2):
            n = 2 * positions[j] + zz
            w = [weights[c, n, :, :, 384:512].reshape(256, 128) for c in range(2)]
            w = jnp.concatenate(w, axis=1)
            share = dot_nt(mixed[...], w).astype(BF16)
            cols = slice(zz * 256, (zz + 1) * 256)
            for h in range(2):
                put_pieces(
                    j, h, share[h * 256 : (h + 1) * 256],
                    *(ref.at[:, cols] for ref in (o_own, o_right, o_left, o_keep_right, o_keep_left)),
                    slice(h * 256, (h + 1) * 256),
                )


def norm_kernel(
    place, t_own, t_left, t_right, t_far, m_own, m_left, m_right, m_low, m_high,
    merge_gain, channel_gain, arrived, normed, o_first, near, sem,
):
    copy = pltpu.make_async_copy(arrived, near, sem)
    copy.start()
    x, k = place[0], place[1]
    positions = [lax.rem(x + j, 4) for j in range(4)]
    base = pl.multiple_of(k * HALO, HALO)
    for i in range(2):

        @pl.loop(0, 4)
        def _(tile):
            at = pl.multiple_of(tile * 64, 64)
            r, h = pl.ds(i * 256 + at, 64), pl.ds(at, 64)
            tr = pl.ds(base + i * 256 + at, 64)
            merged = [b.astype(F32) for b in (m_own[r, :], m_right[r, :], (m_low if i == 0 else m_high)[h, :], m_left[r, :])]
            toks = [b[tr, :].astype(F32) for b in (t_own, t_right, t_far, t_left)]
            squares = sum(jnp.sum(f * f, axis=1, keepdims=True) for f in merged)
            factor = lax.rsqrt(squares * (1.0 / 2048) + EPS)
            first = []
            for j in range(4):
                g = merge_gain[pl.ds(positions[j], 1), :]
                first.append((toks[j] + merged[j] * factor * g).astype(BF16))
            o_first[r, :] = first[0]
            first = [f.astype(F32) for f in first]
            squares = sum(jnp.sum(f * f, axis=1, keepdims=True) for f in first)
            factor = lax.rsqrt(squares * (1.0 / 2048) + EPS)
            for j in range(4):
                g = channel_gain[pl.ds(positions[j], 1), :]
                start = pl.multiple_of(positions[j] * 512, 512)
                normed[r, pl.ds(start, 512)] = (first[j] * factor * g).astype(BF16)

    copy.wait()


def pack_kernel(gate, up, down, out):
    out[:, 0:640] = gate[:, 0:640]
    out[:, 640:1280] = up[:, 0:640]
    out[:, 1280:1408] = jnp.concatenate([gate[:, 640:704], up[:, 640:704]], axis=1)
    out[:, 1408:2048] = down[:, 0:640]
    out[:, 2048:2176] = jnp.concatenate([down[:, 640:704], jnp.zeros((64, 64), BF16)], axis=1)


def gate_rows(normed, weights, hidden):
    lane = lax.broadcasted_iota(jnp.int32, (256, 128), 1)

    @pl.loop(0, 2)
    def _(i):
        r = pl.ds(pl.multiple_of(i * 256, 256), 256)
        both = jnp.dot(normed[r, :], weights[:, 0:1408], preferred_element_type=F32)
        gate, up, tail = both[:, 0:640], both[:, 640:1280], both[:, 1280:1408]
        hidden[r, 0:640] = (gate / (1.0 + jnp.exp(-gate)) * up).astype(BF16)
        last = tail / (1.0 + jnp.exp(-tail)) * pltpu.roll(tail, 64, 1)
        hidden[r, 640:768] = jnp.where(lane < 64, last, 0.0).astype(BF16)


def forward_kernel(place, normed, mine, ready, other, out, fetched, hidden, partial, sem):
    copy = pltpu.make_async_copy(other, fetched, sem)
    copy.start()
    x = place[0]

    def products(left, weights, keep):
        @pl.loop(0, 2)
        def _(i):
            r = pl.ds(pl.multiple_of(i * 256, 256), 256)
            for j in range(4):
                start = pl.multiple_of(lax.rem(x + j, 4) * 512, 512)
                for zz in range(2):
                    share = dot_nt(left[r, :], weights[pl.ds(start + zz * 256, 256), 1408:2176])
                    keep(j, r, slice(zz * 256, (zz + 1) * 256), share)

    def first(j, r, cols, share):
        partial[j, r, cols] = share

    def second(j, r, cols, share):
        out[j, r, cols] = (partial[j, r, cols] + share).astype(BF16)

    products(ready, mine, first)
    copy.wait()
    gate_rows(normed, fetched, hidden)
    products(hidden, fetched, second)


VM = pl.BlockSpec(memory_space=pltpu.VMEM)
SM = pl.BlockSpec(memory_space=pltpu.SMEM)
HB = pl.BlockSpec(memory_space=pltpu.HBM)
SHARES = [
    jax.ShapeDtypeStruct((512, 512), BF16),
    jax.ShapeDtypeStruct((512, 512), BF16),
    jax.ShapeDtypeStruct((512, 512), BF16),
    jax.ShapeDtypeStruct((256, 512), BF16),
    jax.ShapeDtypeStruct((256, 512), BF16),
]


def shards(
    tokens, mixer_gain, conv_taps, outer_weight, inner_weight, value_weight, merge_weight,
    merge_gain, channel_gain, gate_weight, up_weight, down_weight, output_gain,
):
    x, k = lax.axis_index("tp_0"), lax.axis_index("tp_1")
    y = lax.axis_index("fs_1")
    place = jnp.stack([x, k, y]).astype(jnp.int32)
    span = 512 + HALO

    first_weights = jnp.concatenate([outer_weight, inner_weight, value_weight, merge_weight.T], axis=1)
    second_weights = pl.pallas_call(
        pack_kernel, out_shape=jax.ShapeDtypeStruct((64, 2176), BF16), in_specs=[VM] * 3, out_specs=VM
    )(gate_weight, up_weight, down_weight.T)
    second = lax.all_gather(second_weights, FS, axis=0, tiled=True)

    kept = lax.dynamic_slice_in_dim(tokens, k * (512 - HALO), span, 0)
    given = lax.dynamic_slice_in_dim(tokens, (1 - k) * (512 - HALO), span, 0)
    taken = shift(given, "tp_1", 1)
    block = jnp.where(k == 0, jnp.concatenate([kept, taken], 1), jnp.concatenate([taken, kept], 1))
    t_own, t_left, t_right, t_low, t_high = around(block, "tp_0", cut=288)

    plane = copy_for_each(first_weights, "fs_0")
    near = around(plane, "fs_1")
    near_other = [shift(part, "tp_1", 1) for part in near]

    own_taps = lax.dynamic_slice_in_dim(conv_taps, x * 256, 256, 1).astype(F32)
    pieces = pl.pallas_call(
        mixer_kernel,
        out_shape=SHARES,
        in_specs=[SM] + [VM] * 5 + [HB] * 10 + [VM] * 2,
        out_specs=[VM] * 5,
        scratch_shapes=[
            pltpu.VMEM((2, 8, 4, 64, 512), BF16),
            pltpu.VMEM((span, 2048), BF16),
            pltpu.VMEM((span, 256), F32),
            pltpu.VMEM((span + 8, 256), F32),
            pltpu.VMEM((512, 256), BF16),
            pltpu.SemaphoreType.DMA((10,)),
        ],
        compiler_params=pltpu.CompilerParams(vmem_limit_bytes=26 * 2**20),
        cost_estimate=pl.CostEstimate(flops=2_300_000_000, bytes_accessed=9_000_000, transcendentals=0),
    )(place, t_own, t_left, t_right, t_low, t_high, *near, *near_other, own_taps, mixer_gain.reshape(4, 512))
    merged = scatter_sum(*pieces)
    second_other = shift(second, "tp_1", 1)
    gathered = around(merged, "tp_0")

    normed, first, second = pl.pallas_call(
        norm_kernel,
        out_shape=[
            jax.ShapeDtypeStruct((512, 2048), BF16),
            jax.ShapeDtypeStruct((512, 512), BF16),
            jax.ShapeDtypeStruct((2048, 2176), BF16),
        ],
        in_specs=[SM] + [VM] * 11 + [HB],
        out_specs=[VM] * 3,
        scratch_shapes=[pltpu.SemaphoreType.DMA],
        compiler_params=pltpu.CompilerParams(vmem_limit_bytes=32 * 2**20),
        cost_estimate=pl.CostEstimate(flops=30_000_000, bytes_accessed=6_500_000, transcendentals=0),
    )(
        place, t_own, t_left, t_right, jnp.concatenate([t_low, t_high], 0), *gathered,
        merge_gain.reshape(4, 512), channel_gain.reshape(4, 512), second,
    )
    ready = pl.pallas_call(
        gate_rows,
        out_shape=jax.ShapeDtypeStruct((512, 768), BF16),
        in_specs=[VM] * 2,
        out_specs=VM,
        compiler_params=pltpu.CompilerParams(vmem_limit_bytes=20 * 2**20),
        cost_estimate=pl.CostEstimate(flops=3_000_000_000, bytes_accessed=8_000_000, transcendentals=0),
    )(normed, second)
    ours = pl.pallas_call(
        forward_kernel,
        out_shape=jax.ShapeDtypeStruct((4, 512, 512), BF16),
        in_specs=[SM] + [VM] * 3 + [HB],
        out_specs=VM,
        scratch_shapes=[
            pltpu.VMEM((2048, 2176), BF16),
            pltpu.VMEM((512, 768), BF16),
            pltpu.VMEM((4, 512, 512), F32),
            pltpu.SemaphoreType.DMA,
        ],
        compiler_params=pltpu.CompilerParams(vmem_limit_bytes=34 * 2**20),
        cost_estimate=pl.CostEstimate(flops=6_000_000_000, bytes_accessed=13_000_000, transcendentals=0),
    )(place, normed, second, ready, second_other)
    pieces = (
        ours[0],
        jnp.concatenate([ours[2, :256], ours[1, 256:]], 0),
        jnp.concatenate([ours[2, 256:], ours[3, :256]], 0),
        ours[1, :256],
        ours[3, 256:],
    )
    down = scatter_sum(*pieces).astype(F32)
    squares = jnp.sum(down * down, axis=1).reshape(4, 128)
    total = squares + shift(squares, "tp_0", 1) + shift(squares, "tp_0", -1) + shift(squares, "tp_0", 2)
    factor = lax.rsqrt(total.reshape(512, 1) / 2048 + EPS)
    own_gain = lax.dynamic_slice_in_dim(output_gain, x * 512, 512)
    result = (first.astype(F32) + down * factor * own_gain).astype(BF16)
    kept = lax.dynamic_slice_in_dim(result, k * 256, 256, 1)
    given = lax.dynamic_slice_in_dim(result, (1 - k) * 256, 256, 1)
    taken = shift(given, "tp_1", 1)
    return jnp.where(k == 0, jnp.concatenate([kept, taken], 0), jnp.concatenate([taken, kept], 0))


def solution(mesh):
    finer = Mesh(mesh.devices.reshape(8, 4, 4, 2), ("fs_0", "fs_1", "tp_0", "tp_1"))
    wide, tall = P(FS, TP), P(TP, FS)
    placed = (wide, P(), P(), wide, wide, wide, tall, P(), P(), wide, wide, tall, P())
    named = lambda *args: shards(*args)
    return jax.shard_map(named, mesh=finer, in_specs=placed, out_specs=P(FS, TP), check_vma=False)
```
